32 devices in a mesh: sp: 8 (over z, x), tp: 4 (over y, core).
Axes of the slice: x: 2, y: 2, z: 4, core: 2. Of those that a mesh axis runs over, the one named last changes fastest.
Arguments:
- residual_layer_input: bfloat16 [2048, 2048], P(('sp', 'tp')), may hold values from -6 to 6
- value_projected: bfloat16 [2048, 4096], P('sp', 'tp'), may hold values from -6 to 6
- key_projected: bfloat16 [2048, 2048], P('sp', 'tp'), may hold values from -6 to 6
- query_projected: bfloat16 [2048, 2048], P('sp', 'tp'), may hold values from -6 to 6
- output_gate_projected: bfloat16 [2048, 4096], P('sp', 'tp'), may hold values from -6 to 6
- step_projected_raw: bfloat16 [2, 2048, 64], P(None, 'sp', 'tp'), may hold values from -5.5 to 5
- head_decay_logarithm: float32 [2, 64], P(None, 'tp'), may hold values from -15 to -2.9
- position_extra_decay: float32 [2048, 64], P('sp', 'tp'), may hold values from -2.1 to 0
- value_filter_weight: bfloat16 [5, 4096], P(None, 'tp'), may hold values from -2.5 to 2.5
- key_filter_weight: bfloat16 [5, 2048], P(None, 'tp'), may hold values from -2.5 to 2.5
- query_filter_weight: bfloat16 [5, 2048], P(None, 'tp'), may hold values from -2.5 to 2.5
- head_norm_gain: float32 [4096], P('tp'), may hold values from 0.1 to 1.9
- mixer_output_matrix: bfloat16 [4096, 2048], P(None, 'tp'), may hold values from -0.09375 to 0.09375
- expert_norm_gain: float32 [2048], replicated, may hold values from 0.1 to 1.9
- routes: int32 [2048, 2], P('sp'), may hold values from 0 to 7, all different within a row; in each aligned block of 64 rows (0 to 63, 64 to 127, ...) at most 32 rows name the same one
- chosen_expert_weight: float32 [2048, 2], P(('sp', 'tp')), may hold values from 0.1 to 1
- expert_gate_matrix: bfloat16 [8, 2048, 4096], P('sp', None, 'tp'), may hold values from -0.125 to 0.125
- expert_up_matrix: bfloat16 [8, 2048, 4096], P('sp', None, 'tp'), may hold values from -0.125 to 0.125
- expert_down_matrix: bfloat16 [8, 4096, 2048], P('sp', 'tp'), may hold values from -0.09375 to 0.09375
Outputs:
- layer_output: bfloat16 [2048, 2048], P(('sp', 'tp'))
The draws below stay inside these ranges and needn't reach their ends.
Inputs may be any that keep to these rules, and one draw needn't show every extreme that they name: `routes`: each row names 2 different experts; the rows of one device (aligned blocks of 64 rows) name one expert 32 times at most, and that most is reached.
All inputs are finite; a program needn't handle non-finite values.
Results may differ from the reference program's by a relative error of at most 0.015.
Values may be sent and summed in bfloat16 or wider, within the bound.
No kernel may reach another device: no remote copies, remote signals or barrier semaphores. Data moves between devices by JAX's collectives and lax.ppermute only.
A program may use at most 64 MiB of HBM per device.

```python
import math
import jax
import jax.numpy as jnp
import numpy as np
from jax import lax

D = 2048
HEAD_DIM = 64
HEADS = 64
INNER = 4096
GROUPS = 16
STATE = 128
BLOCK = 128
TAPS = 5
EXPERT_FF = 4096
TOP = 2
TOK_DEV = 256
TOKENS = 2048
ROWS_DEV = 64
EXPERTS = 8
CAPACITY = 32
FF_SHARE = 1024
N_TP = 4


def draw_step_projected_raw(key, part):
    noise_key, level_key = jax.random.split(key)
    noise_part = jnp.clip(jax.random.normal(noise_key, (2, TOKENS, HEADS), jnp.float32), -4.0, 4.0)
    segments = TOKENS // TOK_DEV
    first_key, second_key = jax.random.split(level_key)
    ranks = jnp.stack([jax.random.permutation(first_key, segments), jax.random.permutation(second_key, segments)]).astype(jnp.float32)
    shift = -1.5 + 2.5 * ranks / max(segments - 1, 1)
    shift_rows = jnp.repeat(shift, TOK_DEV, axis=1)
    return (noise_part + shift_rows[:, :, None]).astype(jnp.bfloat16)


def draw_head_decay_logarithm(key, part):
    pick_key, fast_key, slow_key = jax.random.split(key, 3)
    fast_share = 0.5
    fast_heads = jax.random.uniform(pick_key, (2, HEADS), jnp.float32) < fast_share
    fast_rate = jnp.exp(jax.random.uniform(fast_key, (2, HEADS), jnp.float32, math.log(1.0 / 60.0), math.log(1.0 / 20.0)))
    slow_rate = jax.random.uniform(slow_key, (2, HEADS), jnp.float32, 0.05, 0.6) / TOKENS
    return jnp.log(jnp.where(fast_heads, fast_rate, slow_rate)).astype(jnp.float32)


def draw_position_extra_decay(key, part):
    place_key, depth_key = jax.random.split(key)
    spots = jax.random.randint(place_key, (3,), 0, TOKENS)
    depth = jnp.log(jax.random.uniform(depth_key, (3, HEADS), jnp.float32, 0.5, 0.8))
    matches = (lax.broadcasted_iota(jnp.int32, (TOKENS, 3), 0) == spots[None, :]).astype(jnp.float32)
    return jnp.dot(matches, depth, precision=lax.Precision.HIGHEST).astype(jnp.float32)


def steps_of(rng, shape, cuts, smallest, high):
    loudness = 1.0
    for dim, parts in cuts:
        draws = jax.random.uniform(jax.random.fold_in(jax.random.fold_in(rng, 6), dim), (parts,), jnp.float32, smallest / len(cuts), high / len(cuts))
        loudness = loudness * jnp.repeat(jnp.exp(draws), shape[dim] // parts).reshape((-1,) + (1,) * (len(shape) - 1 - dim))
    return loudness


def routed_block(stream_key, own, number, rows, number_of, top, bound, skew):
    sequence = jax.random.permutation(stream_key, number_of)
    crowded, common = shares(number_of, rows * top, bound, skew, True), shares(number_of, rows * top, bound, skew, False)
    places = jnp.arange(number_of)

    def named(tallies, rotation):
        used = int((tallies > 0).sum())
        fixed = max(1, used // 4)
        moved = fixed + (places - fixed + rotation * (used - fixed)) % max(1, number_of - fixed)
        return jnp.zeros((number_of,), jnp.int32).at[sequence[jnp.where(places < fixed, places, moved)]].set(jnp.asarray(tallies, jnp.int32))

    tallies = jnp.where(number % 4 == 0, named(crowded, number // 4), named(common, number - number // 4 - 1))
    mixed = jax.random.permutation(jax.random.fold_in(own, 3), number_of)
    giver, taker = mixed[0:number_of // 2 * 2:2], mixed[1:number_of // 2 * 2:2]
    room = jnp.minimum(tallies[giver] - 1, bound - tallies[taker]) // 2
    room = jnp.where((giver == sequence[0]) | (taker == sequence[0]) | (tallies[taker] == 0), 0, jnp.maximum(room, 0))
    moved = jax.random.randint(jax.random.fold_in(own, 4), (number_of // 2,), 0, 1 << 20) % (room + 1)
    tallies = tallies.at[giver].add(-moved).at[taker].add(moved)
    labels = jnp.searchsorted(jnp.cumsum(tallies), jnp.arange(rows * top), side="right").astype(jnp.int32)
    grid = labels.reshape(top, rows).T
    grid = grid[jax.random.permutation(jax.random.fold_in(own, 1), rows)]
    rotation = jax.random.randint(jax.random.fold_in(own, 2), (rows, 1), 0, top)
    return jnp.take_along_axis(grid, (jnp.arange(top)[None, :] + rotation) % top, axis=1)


def shares(count, total, reach, lean, full):
    loads = [(1 << 20) // math.isqrt(rank ** lean) + 1 for rank in range(1, count + 1)]
    largest = reach if full else min(reach, max(-(-total // count), total * loads[0] // sum(loads)))
    least = 1 if total - largest >= count - 1 else 0
    counts, surplus = [largest] + [least] * (count - 1), total - largest - least * (count - 1)
    while surplus > 0:
        candidates = [i for i in range(1, count) if counts[i] < largest] or [i for i in range(1, count) if counts[i] < reach]
        whole, remaining = sum([loads[i] for i in candidates]), surplus
        for i in candidates:
            extra = min(reach - counts[i], max(1, remaining * loads[i] // whole), surplus)
            counts[i] = counts[i] + extra
            surplus = surplus - extra
    return np.array(counts)


def gaussian(stream_key, dims, scale, reach, shards=(), held_as=jnp.bfloat16):
    values = scale * jax.random.normal(stream_key, dims, jnp.float32)
    if shards:
        values = values * steps_of(stream_key, dims, shards, -0.22, 0.18)
    return jnp.clip(values, -reach, reach).astype(held_as)


def setup_inputs(seed: int = 0) -> dict:
    arg_keys = jax.random.split(jax.random.key(seed), 20)
    residual_layer_input = gaussian(arg_keys[0], (TOKENS, D), 1.0, 6.0, ((0, 32),))
    value_projected = gaussian(arg_keys[1], (TOKENS, INNER), 1.0, 6.0, ((0, 8), (1, 4)))
    key_projected = gaussian(arg_keys[2], (TOKENS, GROUPS * STATE), 1.0, 6.0, ((0, 8), (1, 4)))
    query_projected = gaussian(arg_keys[3], (TOKENS, GROUPS * STATE), 1.0, 6.0, ((0, 8), (1, 4)))
    output_gate_projected = gaussian(arg_keys[4], (TOKENS, INNER), 1.0, 6.0, ((0, 8), (1, 4)))
    step_projected_raw = draw_step_projected_raw(jax.random.fold_in(arg_keys[19], 71), 0)
    head_decay_logarithm = draw_head_decay_logarithm(jax.random.fold_in(arg_keys[19], 71), 0)
    position_extra_decay = draw_position_extra_decay(jax.random.fold_in(arg_keys[19], 71), 0)
    value_filter_weight = gaussian(arg_keys[8], (TAPS, INNER), TAPS ** -0.5, 2.5, ((1, 4),))
    key_filter_weight = gaussian(arg_keys[9], (TAPS, GROUPS * STATE), TAPS ** -0.5, 2.5, ((1, 4),))
    query_filter_weight = gaussian(arg_keys[10], (TAPS, GROUPS * STATE), TAPS ** -0.5, 2.5, ((1, 4),))
    head_norm_gain = jnp.clip(1.0 + 0.18 * jax.random.normal(arg_keys[11], (INNER,), jnp.float32), 0.1, 1.9)
    mixer_output_matrix = gaussian(arg_keys[12], (INNER, D), INNER ** -0.5, 0.09375, ((1, 4),))
    expert_norm_gain = jnp.clip(1.0 + 0.18 * jax.random.normal(arg_keys[13], (D,), jnp.float32), 0.1, 1.9)
    routes_keys = jax.random.split(jax.random.fold_in(arg_keys[14], 1), TOKENS // ROWS_DEV)
    routes_turns = jax.random.permutation(jax.random.fold_in(arg_keys[14], 3), TOKENS // ROWS_DEV)
    routes = jax.vmap(lambda own, number: routed_block(jax.random.fold_in(arg_keys[14], 2), own, number, ROWS_DEV, EXPERTS, TOP, CAPACITY, 1))(routes_keys, routes_turns).reshape((TOKENS, TOP))
    chosen_expert_weight = jnp.clip(0.1 + 0.9 * jax.random.uniform(arg_keys[15], (TOKENS, TOP), jnp.float32) ** steps_of(arg_keys[15], (TOKENS, TOP), ((0, 32),), -0.2, 0.2), 0.1, 1.0)
    expert_gate_matrix = gaussian(arg_keys[16], (EXPERTS, D, EXPERT_FF), D ** -0.5, 0.125, ((0, 8), (2, 4)))
    expert_up_matrix = gaussian(arg_keys[17], (EXPERTS, D, EXPERT_FF), D ** -0.5, 0.125, ((0, 8), (2, 4)))
    expert_down_matrix = gaussian(arg_keys[18], (EXPERTS, EXPERT_FF, D), EXPERT_FF ** -0.5, 0.09375, ((0, 8), (1, 4)))
    return {"residual_layer_input": residual_layer_input, "value_projected": value_projected, "key_projected": key_projected, "query_projected": query_projected, "output_gate_projected": output_gate_projected, "step_projected_raw": step_projected_raw, "head_decay_logarithm": head_decay_logarithm, "position_extra_decay": position_extra_decay, "value_filter_weight": value_filter_weight, "key_filter_weight": key_filter_weight, "query_filter_weight": query_filter_weight, "head_norm_gain": head_norm_gain, "mixer_output_matrix": mixer_output_matrix, "expert_norm_gain": expert_norm_gain, "routes": routes, "chosen_expert_weight": chosen_expert_weight, "expert_gate_matrix": expert_gate_matrix, "expert_up_matrix": expert_up_matrix, "expert_down_matrix": expert_down_matrix}


epsilon = 1e-06

def centred_taps(inputs, taps):
    length = inputs.shape[0]
    half_width = (taps.shape[0] - 1) // 2
    padded = jnp.pad(inputs.astype(jnp.float32), ((half_width, half_width), (0, 0)))
    weights = taps.astype(jnp.float32)
    result = weights[0] * padded[0:length]
    for offset in range(1, taps.shape[0]):
        result = result + weights[offset] * padded[offset:offset + length]
    return result

def block_terms(operands):
    forward_cum, backward_excl, forward_part, backward_part, key_rows, query_rows = operands
    scores = jnp.einsum('lgn,sgn->lsg', query_rows.astype(jnp.float32), key_rows.astype(jnp.float32))
    position = jnp.arange(scores.shape[0], dtype=jnp.int32)
    lower_mask = (position[None, :] <= position[:, None])[:, :, None, None]
    upper_mask = (position[None, :] >= position[:, None])[:, :, None, None]
    forward_gap = jnp.where(lower_mask, forward_cum[:, None] - forward_cum[None, :], -jnp.inf)
    backward_gap = jnp.where(upper_mask, backward_excl[None, :] - backward_excl[:, None], -jnp.inf)
    forward_weight = (scores[..., None] * jnp.exp(forward_gap)).astype(jnp.bfloat16)
    backward_weight = (scores[..., None] * jnp.exp(backward_gap)).astype(jnp.bfloat16)
    inner = jnp.einsum('lsgh,sghp->lghp', forward_weight.astype(jnp.float32), forward_part.astype(jnp.float32))
    inner = inner + jnp.einsum('lsgh,sghp->lghp', backward_weight.astype(jnp.float32), backward_part.astype(jnp.float32))
    key_wide = key_rows.astype(jnp.float32)[:, :, None, :]
    forward_keys = (jnp.exp(forward_cum[-1][None] - forward_cum)[..., None] * key_wide).astype(jnp.bfloat16)
    backward_keys = (jnp.exp(backward_excl)[..., None] * key_wide).astype(jnp.bfloat16)
    forward_state = jnp.einsum('sghn,sghp->ghpn', forward_keys.astype(jnp.float32), forward_part.astype(jnp.float32))
    backward_state = jnp.einsum('sghn,sghp->ghpn', backward_keys.astype(jnp.float32), backward_part.astype(jnp.float32))
    return (inner, forward_state, backward_state)

def advance(carried, operands):
    block_state, block_total = operands
    return (jnp.exp(block_total)[..., None, None] * carried + block_state, carried)

def apply_expert(operands):
    slot_block, gate_part, up_part, down_part = operands
    gate_value = jnp.dot(slot_block, gate_part, preferred_element_type=jnp.float32)
    up_value = jnp.dot(slot_block, up_part, preferred_element_type=jnp.float32)
    hidden = (jax.nn.silu(gate_value) * up_value).astype(jnp.bfloat16)
    pieces = jnp.einsum('rjf,jfd->jrd', hidden.reshape(slot_block.shape[0], N_TP, FF_SHARE).astype(jnp.float32), down_part.reshape(N_TP, FF_SHARE, D).astype(jnp.float32)).astype(jnp.bfloat16)
    return lax.optimization_barrier(jnp.sum(pieces.astype(jnp.float32), axis=0)).astype(jnp.bfloat16)

def reference(residual_layer_input, value_projected, key_projected, query_projected, output_gate_projected, step_projected_raw, head_decay_logarithm, position_extra_decay, value_filter_weight, key_filter_weight, query_filter_weight, head_norm_gain, mixer_output_matrix, expert_norm_gain, routes, chosen_expert_weight, expert_gate_matrix, expert_up_matrix, expert_down_matrix):
    tokens = value_projected.shape[0]
    per_group = HEADS // GROUPS
    blocks = tokens // BLOCK
    values = centred_taps(value_projected, value_filter_weight).astype(jnp.bfloat16)
    key_rows = jax.nn.silu(centred_taps(key_projected, key_filter_weight)).astype(jnp.bfloat16).reshape(blocks, BLOCK, GROUPS, STATE)
    query_rows = jax.nn.silu(centred_taps(query_projected, query_filter_weight)).astype(jnp.bfloat16).reshape(blocks, BLOCK, GROUPS, STATE)
    positive_step_sizes = jax.nn.softplus(step_projected_raw.astype(jnp.float32))
    decay_logarithm = -jnp.exp(head_decay_logarithm)[:, None, :] * positive_step_sizes + position_extra_decay[None]
    scaled = (values.astype(jnp.float32).reshape(tokens, HEADS, HEAD_DIM)[None] * positive_step_sizes[..., None]).astype(jnp.bfloat16)
    scaled = scaled.reshape(2, blocks, BLOCK, GROUPS, per_group, HEAD_DIM)
    log_blocks = decay_logarithm.reshape(2, blocks, BLOCK, GROUPS, per_group)
    running = jnp.cumsum(log_blocks, axis=2)
    forward_cum = running[0]
    backward_excl = running[1] - log_blocks[1]
    forward_total = running[0][:, -1]
    backward_total = running[1][:, -1]
    inner, forward_state, backward_state = lax.map(block_terms, (forward_cum, backward_excl, scaled[0], scaled[1], key_rows, query_rows))
    zero_state = jnp.zeros((GROUPS, per_group, HEAD_DIM, STATE), jnp.float32)
    entering = lax.scan(advance, zero_state, (forward_state, forward_total))[1]
    leaving = lax.scan(advance, zero_state, (backward_state, backward_total), reverse=True)[1]
    query_wide = query_rows.astype(jnp.float32)
    forward_read = jnp.exp(forward_cum)[..., None] * jnp.einsum('blgn,bghpn->blghp', query_wide, entering.astype(jnp.bfloat16).astype(jnp.float32))
    backward_read = jnp.exp(backward_total[:, None] - backward_excl)[..., None] * jnp.einsum('blgn,bghpn->blghp', query_wide, leaving.astype(jnp.bfloat16).astype(jnp.float32))
    mixer_raw = (inner + forward_read + backward_read).reshape(tokens, HEADS, HEAD_DIM)
    gated = mixer_raw * jax.nn.silu(output_gate_projected.astype(jnp.float32)).reshape(tokens, HEADS, HEAD_DIM)
    inverse_rms = lax.rsqrt(lax.optimization_barrier(jnp.mean(gated * gated, axis=-1, keepdims=True)) + epsilon)
    head_normed = (gated * inverse_rms * head_norm_gain.reshape(HEADS, HEAD_DIM)).astype(jnp.bfloat16)
    head_normed = head_normed.reshape(tokens, HEADS * HEAD_DIM)
    mixer_out = jnp.dot(head_normed, mixer_output_matrix, preferred_element_type=jnp.float32).astype(jnp.bfloat16)
    middle = (residual_layer_input.astype(jnp.float32) + mixer_out.astype(jnp.float32)).astype(jnp.bfloat16)
    residual = middle.astype(jnp.float32)
    normed = (residual * lax.rsqrt(lax.optimization_barrier(jnp.mean(residual * residual, axis=-1, keepdims=True)) + epsilon) * expert_norm_gain).astype(jnp.bfloat16)
    device_blocks = tokens // ROWS_DEV
    slots_each = device_blocks * CAPACITY
    flat_routes = routes.reshape(device_blocks, ROWS_DEV * TOP).astype(jnp.int32)
    matches = (flat_routes[:, :, None] == jnp.arange(EXPERTS, dtype=jnp.int32)[None, None, :]).astype(jnp.int32)
    earlier = (jnp.cumsum(matches, axis=1) - matches).astype(jnp.int32)
    rank_in = lax.optimization_barrier(jnp.sum(matches * earlier, axis=2)).astype(jnp.int32)
    block_index = jnp.arange(device_blocks, dtype=jnp.int32)[:, None]
    slot_ids = (flat_routes * slots_each + block_index * CAPACITY + rank_in).reshape(-1).astype(jnp.int32)
    copies = jnp.repeat(normed, TOP, axis=0)
    slot_rows = jnp.zeros((EXPERTS * slots_each, D), jnp.bfloat16).at[slot_ids].set(copies)
    expert_out = lax.map(apply_expert, (slot_rows.reshape(EXPERTS, slots_each, D), expert_gate_matrix, expert_up_matrix, expert_down_matrix))
    picked = expert_out.reshape(EXPERTS * slots_each, D)[slot_ids].astype(jnp.float32).reshape(tokens, TOP, D)
    expert_mix = lax.optimization_barrier(jnp.sum(picked * chosen_expert_weight[:, :, None], axis=1))
    return (residual + expert_mix).astype(jnp.bfloat16)
```

```python
import jax
import jax.numpy as jnp
from jax import lax
from jax.sharding import PartitionSpec as P

HEAD_DIM = 64
STATE = 128
BLOCK = 128
TAPS = 5


epsilon = 1e-06
highest = lax.Precision.HIGHEST


def padded_2(cells, sides, width):
    for axis, dim in sides:
        count = lax.axis_size(axis)
        ends = count - 1
        head = lax.slice_in_dim(cells, 0, width, axis=dim)
        tail = lax.slice_in_dim(cells, cells.shape[dim] - width, cells.shape[dim], axis=dim)
        cells = jnp.concatenate(
            [
                lax.ppermute(tail, axis, [(i, (i + 1) % count) for i in range(ends)]),
                cells,
                lax.ppermute(head, axis, [((i + 1) % count, i) for i in range(ends)]),
            ],
            axis=dim,
        )
    return cells


def carried_states(totals, states):
    count = lax.axis_size("sp")
    heads = totals.shape[1]
    _, depth, columns = states.shape
    decay = jnp.exp(totals).reshape(1, 2 * heads)
    high = decay.astype(jnp.bfloat16)
    low = (decay - high.astype(jnp.float32)).astype(jnp.bfloat16)
    extra = jnp.broadcast_to(jnp.concatenate([high, low], axis=1), (depth, 4 * heads))
    sent = jnp.concatenate(
        [states[0].astype(jnp.bfloat16), states[1].astype(jnp.bfloat16), extra], axis=1
    )
    sent = sent.reshape(count, depth // count, sent.shape[1])
    arrived = lax.all_to_all(sent, "sp", split_axis=0, concat_axis=0, tiled=True)
    rows = arrived.astype(jnp.float32)
    tail = rows[:, 0, 2 * columns :]
    decays = jnp.repeat(tail[:, : 2 * heads] + tail[:, 2 * heads :], columns // heads, axis=1)
    entering = [jnp.zeros((depth // count, columns), jnp.float32)]
    leaving = [jnp.zeros((depth // count, columns), jnp.float32)]
    for k in range(count - 1):
        entering.append(entering[-1] * decays[k, :columns] + rows[k, :, :columns])
        back = count - 1 - k
        leaving.append(leaving[-1] * decays[back, columns:] + rows[back, :, columns : 2 * columns])
    answer = jnp.stack(
        [
            jnp.concatenate([a, b], axis=1)
            for a, b in zip(entering, leaving[::-1])
        ]
    ).astype(jnp.bfloat16)
    back = lax.all_to_all(answer, "sp", split_axis=0, concat_axis=0, tiled=True)
    back = back.reshape(depth, 2 * columns).astype(jnp.float32)
    return back[:, :columns], back[:, columns:]


def prefix_matrix(length):
    row_index = lax.broadcasted_iota(jnp.int32, (length, length), 0)
    column_index = lax.broadcasted_iota(jnp.int32, (length, length), 1)
    return (column_index <= row_index).astype(jnp.float32)


def local_chain(states, totals, reverse):

    def advance(carried, operands):
        block_state, block_total = operands
        return (jnp.exp(block_total)[..., None, None] * carried + block_state, carried)

    start_state = jnp.zeros(states.shape[1:], jnp.float32)
    return lax.scan(advance, start_state, (states, totals), reverse=reverse)


def mix_tokens(
    value_projected,
    key_projected,
    query_projected,
    output_gate_projected,
    step_projected_raw,
    head_decay_logarithm,
    position_extra_decay,
    value_filter_weight,
    key_filter_weight,
    query_filter_weight,
    head_norm_gain,
):
    tokens = value_projected.shape[0]
    value_width = value_projected.shape[1]
    key_width = key_projected.shape[1]
    head_count = step_projected_raw.shape[2]
    group_count = key_width // STATE
    per_group = head_count // group_count
    blocks = tokens // BLOCK
    joined = jnp.concatenate([value_projected, key_projected, query_projected], axis=1)
    padded = padded_2(joined, (("sp", 0),), (TAPS - 1) // 2).astype(jnp.float32)
    weights = jnp.concatenate(
        [value_filter_weight, key_filter_weight, query_filter_weight], axis=1
    ).astype(jnp.float32)
    filtered = weights[0] * padded[0:tokens]
    for offset in range(1, TAPS):
        filtered = filtered + weights[offset] * padded[offset : offset + tokens]
    values = filtered[:, :value_width].astype(jnp.bfloat16)
    key_rows = jax.nn.silu(filtered[:, value_width : value_width + key_width]).astype(jnp.bfloat16)
    key_rows = key_rows.reshape(blocks, BLOCK, group_count, STATE)
    query_rows = jax.nn.silu(filtered[:, value_width + key_width :]).astype(jnp.bfloat16)
    query_rows = query_rows.reshape(blocks, BLOCK, group_count, STATE)
    positive_step_sizes = jax.nn.softplus(step_projected_raw.astype(jnp.float32))
    decay_logarithm = (
        -jnp.exp(head_decay_logarithm)[:, None, :] * positive_step_sizes
        + position_extra_decay[None]
    )
    scaled = (
        values.astype(jnp.float32).reshape(tokens, head_count, HEAD_DIM)[None]
        * positive_step_sizes[..., None]
    ).astype(jnp.bfloat16)
    scaled = scaled.reshape(2, blocks, BLOCK, group_count, per_group, HEAD_DIM)
    log_blocks = decay_logarithm.reshape(2, blocks, BLOCK, group_count, per_group)
    running = jnp.einsum("ls,dbsgh->dblgh", prefix_matrix(BLOCK), log_blocks, precision=highest)
    forward_cum = running[0]
    backward_excl = running[1] - log_blocks[1]
    forward_total = running[0][:, -1]
    backward_total = running[1][:, -1]
    scores = jnp.einsum("blgn,bsgn->blsg", query_rows, key_rows, preferred_element_type=jnp.float32)
    position = lax.broadcasted_iota(jnp.int32, (BLOCK,), 0)
    lower_mask = (position[None, :] <= position[:, None])[None, :, :, None, None]
    upper_mask = (position[None, :] >= position[:, None])[None, :, :, None, None]
    forward_gap = jnp.where(lower_mask, forward_cum[:, :, None] - forward_cum[:, None, :], -jnp.inf)
    backward_gap = jnp.where(
        upper_mask, backward_excl[:, None, :] - backward_excl[:, :, None], -jnp.inf
    )
    forward_weight = (scores[..., None] * jnp.exp(forward_gap)).astype(jnp.bfloat16)
    backward_weight = (scores[..., None] * jnp.exp(backward_gap)).astype(jnp.bfloat16)
    inner = jnp.einsum(
        "blsgh,bsghp->blghp", forward_weight, scaled[0], preferred_element_type=jnp.float32
    )
    inner = inner + jnp.einsum(
        "blsgh,bsghp->blghp", backward_weight, scaled[1], preferred_element_type=jnp.float32
    )
    key_wide = key_rows.astype(jnp.float32)[:, :, :, None, :]
    forward_keys = (jnp.exp(forward_total[:, None] - forward_cum)[..., None] * key_wide).astype(
        jnp.bfloat16
    )
    backward_keys = (jnp.exp(backward_excl)[..., None] * key_wide).astype(jnp.bfloat16)
    forward_state = jnp.einsum(
        "bsghn,bsghp->bghpn", forward_keys, scaled[0], preferred_element_type=jnp.float32
    )
    backward_state = jnp.einsum(
        "bsghn,bsghp->bghpn", backward_keys, scaled[1], preferred_element_type=jnp.float32
    )
    forward_final, forward_before = local_chain(forward_state, forward_total, False)
    backward_final, backward_before = local_chain(backward_state, backward_total, True)
    forward_sum = jnp.sum(forward_total, axis=0)
    backward_sum = jnp.sum(backward_total, axis=0)
    to_columns = lambda x: x.reshape(-1, STATE).T
    to_states = lambda x: x.T.reshape(forward_final.shape)
    entering, leaving = carried_states(
        jnp.stack([forward_sum.reshape(-1), backward_sum.reshape(-1)]),
        jnp.stack([to_columns(forward_final), to_columns(backward_final)]),
    )
    entering, leaving = to_states(entering), to_states(leaving)
    forward_prior = jnp.cumsum(forward_total, axis=0) - forward_total
    backward_after = backward_sum[None] - jnp.cumsum(backward_total, axis=0)
    forward_in = jnp.exp(forward_prior)[..., None, None] * entering[None] + forward_before
    backward_in = jnp.exp(backward_after)[..., None, None] * leaving[None] + backward_before
    forward_read = jnp.exp(forward_cum)[..., None] * jnp.einsum(
        "blgn,bghpn->blghp",
        query_rows,
        forward_in.astype(jnp.bfloat16),
        preferred_element_type=jnp.float32,
    )
    backward_read = jnp.exp(backward_total[:, None] - backward_excl)[..., None] * jnp.einsum(
        "blgn,bghpn->blghp",
        query_rows,
        backward_in.astype(jnp.bfloat16),
        preferred_element_type=jnp.float32,
    )
    mixer_raw = (inner + forward_read + backward_read).reshape(tokens, head_count, HEAD_DIM)
    gated = mixer_raw * jax.nn.silu(output_gate_projected.astype(jnp.float32)).reshape(
        tokens, head_count, HEAD_DIM
    )
    inverse_rms = lax.rsqrt(jnp.mean(gated * gated, axis=-1, keepdims=True) + epsilon)
    head_normed = (gated * inverse_rms * head_norm_gain.reshape(head_count, HEAD_DIM)).astype(
        jnp.bfloat16
    )
    return head_normed.reshape(tokens, head_count * HEAD_DIM)


def exchange(x, axis, distance):
    count = lax.axis_size(axis)
    return lax.ppermute(x, axis, [(i, i ^ distance) for i in range(count)])


def bits_of(count):
    return [1 << k for k in range(count.bit_length() - 1)]


def gather_rows(rows, axis):
    blocks = rows[None]
    order = [0]
    for bit in reversed(bits_of(lax.axis_size(axis))):
        blocks = jnp.concatenate([blocks, exchange(blocks, axis, bit)], axis=0)
        order = order + [b ^ bit for b in order]
    return blocks, order


def scatter_rows(blocks, axis):
    for bit in bits_of(lax.axis_size(axis)):
        half = blocks.shape[0] // 2
        received = exchange(blocks[half:], axis, bit)
        blocks = (blocks[:half].astype(jnp.float32) + received.astype(jnp.float32)).astype(
            jnp.bfloat16
        )
    return blocks[0]


def slot_table(route_rows, experts, capacity, here):
    flat_ids = route_rows.reshape(-1)
    expert_ids = lax.broadcasted_iota(jnp.int32, (flat_ids.shape[0], experts), 1)
    matches = (flat_ids[:, None] == expert_ids).astype(jnp.float32)
    below = prefix_matrix(flat_ids.shape[0]).astype(jnp.bfloat16)
    running = jnp.dot(
        below, matches.astype(jnp.bfloat16), preferred_element_type=jnp.float32
    )
    rank_in = (jnp.sum(matches * running, axis=1) - 1.0).astype(jnp.int32)
    return ((flat_ids ^ here) * capacity + rank_in).reshape(route_rows.shape)


def reduce_columns(heads_out, own_columns, width):
    axis = "tp"
    count = lax.axis_size(axis)
    me = lax.axis_index(axis)
    blocks = [
        jnp.dot(heads_out, part, preferred_element_type=jnp.float32).astype(jnp.bfloat16)
        for part in own_columns
    ]
    rows = heads_out.shape[0] // count
    partial = jnp.stack([b.reshape(count, rows, width) for b in blocks], axis=2)
    for bit in bits_of(count):
        half = partial.shape[0] // 2
        pairs = partial.reshape(half, 2, rows, count, width)
        mine = (me // bit) % 2
        send = lax.dynamic_index_in_dim(pairs, 1 - mine, 1, keepdims=False)
        keep = lax.dynamic_index_in_dim(pairs, mine, 1, keepdims=False)
        received = exchange(send, axis, bit)
        received = jnp.stack([received[:, :, c ^ bit] for c in range(count)], axis=2)
        partial = (keep.astype(jnp.float32) + received.astype(jnp.float32)).astype(jnp.bfloat16)
    final = partial[0]
    for bit in bits_of(count):
        swapped = jnp.stack([final[:, c ^ bit] for c in range(count)], axis=1)
        final = jnp.where((me // bit) % 2 == 1, swapped, final)
    return final.reshape(rows, count * width)


def own_row_blocks(matrix, rows):
    me = lax.axis_index("tp")
    parts = []
    for t in range(lax.axis_size("tp")):
        block = lax.dynamic_slice_in_dim(matrix, (me ^ t) * rows, rows, 0)
        parts.append(exchange(block, "tp", t) if t else block)
    return parts


def chunks_of(experts):
    quarter = max(experts // 4, 1)
    return [range(0, 2 * quarter), range(2 * quarter, 3 * quarter), range(3 * quarter, experts)]


def shards(
    residual_layer_input,
    value_projected,
    key_projected,
    query_projected,
    output_gate_projected,
    step_projected_raw,
    head_decay_logarithm,
    position_extra_decay,
    value_filter_weight,
    key_filter_weight,
    query_filter_weight,
    head_norm_gain,
    mixer_output_matrix,
    expert_norm_gain,
    routes,
    chosen_expert_weight,
    expert_gate_matrix,
    expert_up_matrix,
    expert_down_matrix,
):
    experts = lax.axis_size("sp")
    here = lax.axis_index("sp")
    position = lax.axis_index("tp")
    own_rows, model_width = residual_layer_input.shape
    top_count = routes.shape[1]
    capacity = 2 * own_rows * top_count // experts
    places = experts * capacity
    own_columns = own_row_blocks(mixer_output_matrix, value_projected.shape[1])
    own_routes = lax.dynamic_slice_in_dim(routes, position * own_rows, own_rows, 0)
    own_slots = slot_table(own_routes, experts, capacity, here)
    place_ids = lax.broadcasted_iota(jnp.int32, (places,) + own_slots.shape, 0)
    one_hot = jnp.sum((place_ids == own_slots[None]).astype(jnp.float32), axis=2).astype(
        jnp.bfloat16
    )
    chosen = (
        lax.broadcasted_iota(jnp.int32, (own_rows, top_count, places), 2) == own_slots[:, :, None]
    )
    mixing = jnp.sum(jnp.where(chosen, chosen_expert_weight[:, :, None], 0.0), axis=1)
    mixing_high = mixing.astype(jnp.bfloat16)
    mixing_low = (mixing - mixing_high.astype(jnp.float32)).astype(jnp.bfloat16)

    heads_out = mix_tokens(
        value_projected,
        key_projected,
        query_projected,
        output_gate_projected,
        step_projected_raw,
        head_decay_logarithm,
        position_extra_decay,
        value_filter_weight,
        key_filter_weight,
        query_filter_weight,
        head_norm_gain,
    )
    mixer_out = reduce_columns(heads_out, own_columns, mixer_output_matrix.shape[1])
    middle = (residual_layer_input.astype(jnp.float32) + mixer_out.astype(jnp.float32)).astype(
        jnp.bfloat16
    )
    residual = middle.astype(jnp.float32)
    normed = (
        residual
        * lax.rsqrt(jnp.mean(residual * residual, axis=-1, keepdims=True) + epsilon)
        * expert_norm_gain
    ).astype(jnp.bfloat16)
    outgoing = jnp.dot(one_hot, normed, preferred_element_type=jnp.float32).astype(jnp.bfloat16)
    outgoing = outgoing.reshape(experts, capacity, model_width)
    returned = []
    for chunk in chunks_of(experts):
        arrived = [exchange(outgoing[d], "sp", d) if d else outgoing[d] for d in chunk]
        blocks, _ = gather_rows(jnp.concatenate(arrived, axis=0), "tp")
        slot_rows = blocks.reshape(-1, model_width)
        gate_value = jnp.dot(slot_rows, expert_gate_matrix[0], preferred_element_type=jnp.float32)
        up_value = jnp.dot(slot_rows, expert_up_matrix[0], preferred_element_type=jnp.float32)
        hidden = (jax.nn.silu(gate_value) * up_value).astype(jnp.bfloat16)
        partial_sum = jnp.dot(
            hidden, expert_down_matrix[0], preferred_element_type=jnp.float32
        ).astype(jnp.bfloat16)
        summed = scatter_rows(partial_sum.reshape(blocks.shape), "tp")
        results = summed.reshape(len(chunk), capacity, model_width)
        returned += [
            exchange(results[i], "sp", d) if d else results[i] for i, d in enumerate(chunk)
        ]
    returned = jnp.concatenate(returned, axis=0)
    expert_mix = jnp.dot(mixing_high, returned, preferred_element_type=jnp.float32)
    expert_mix = expert_mix + jnp.dot(mixing_low, returned, preferred_element_type=jnp.float32)
    return (residual + expert_mix).astype(jnp.bfloat16)


def solution(mesh):
    return jax.shard_map(
        shards,
        mesh=mesh,
        in_specs=(
            P(("sp", "tp"), None),
            P("sp", "tp"),
            P("sp", "tp"),
            P("sp", "tp"),
            P("sp", "tp"),
            P(None, "sp", "tp"),
            P(None, "tp"),
            P("sp", "tp"),
            P(None, "tp"),
            P(None, "tp"),
            P(None, "tp"),
            P("tp"),
            P(None, "tp"),
            P(),
            P("sp", None),
            P(("sp", "tp"), None),
            P("sp", None, "tp"),
            P("sp", None, "tp"),
            P("sp", "tp", None),
        ),
        out_specs=P(("sp", "tp"), None),
        check_vma=False,
    )
```

```python
import functools

import jax
import jax.numpy as jnp
from jax import lax
from jax.experimental import pallas as pl
from jax.experimental.pallas import tpu as pltpu
from jax.sharding import PartitionSpec as P


HEAD_DIM = 64
STATE = 128
TAPS = 5
HALF = (TAPS - 1) // 2
LANES = 128
SUBLANES = 8

epsilon = 1e-06
highest = lax.Precision.HIGHEST
f32 = jnp.float32
bf16 = jnp.bfloat16


def exchange(x, axis, distance):
    count = lax.axis_size(axis)
    return lax.ppermute(x, axis, [(i, i ^ distance) for i in range(count)])


def bits_of(count):
    return [1 << k for k in range(count.bit_length() - 1)]


def butterfly_order(count):
    order = [0]
    for bit in reversed(bits_of(count)):
        order = order + [b ^ bit for b in order]
    return order


def gather_rows(rows, axis):
    blocks = rows[None]
    for bit in reversed(bits_of(lax.axis_size(axis))):
        received = exchange(blocks, axis, bit)
        blocks = jnp.concatenate([blocks, received], axis=0)
    return blocks


def add_rounded(a, b):
    return (a.astype(f32) + b.astype(f32)).astype(bf16)


def scatter_rows(blocks, axis):
    for bit in bits_of(lax.axis_size(axis)):
        half = blocks.shape[0] // 2
        received = exchange(blocks[half:], axis, bit)
        blocks = add_rounded(blocks[:half], received)
    return blocks[0]


def prefix_matrix(length):
    row_index = lax.broadcasted_iota(jnp.int32, (length, length), 0)
    column_index = lax.broadcasted_iota(jnp.int32, (length, length), 1)
    return (column_index <= row_index).astype(f32)


def parts_of(x, count):
    terms = []
    for _ in range(count):
        terms.append(x.astype(bf16))
        x = x - terms[-1].astype(f32)
    return jnp.concatenate(terms, axis=1)


def halo_rows(parts):
    count = lax.axis_size("sp")
    pairs = [(i, i + 1) for i in range(count - 1)]
    tail = jnp.concatenate([p[p.shape[0] - HALF :] for p in parts], axis=1)
    head = jnp.concatenate([p[:HALF] for p in parts], axis=1)
    before = lax.ppermute(tail, "sp", pairs)
    after = lax.ppermute(head, "sp", [(b, a) for a, b in pairs])
    return before, after


def pick_heads(terms, heads, group, per_group, width, count):
    rows = lax.broadcasted_iota(jnp.int32, (count * heads, per_group * width), 0)
    columns = lax.broadcasted_iota(jnp.int32, (count * heads, per_group * width), 1)
    head = rows
    for _ in range(count - 1):
        head = jnp.where(head >= heads, head - heads, head)
    wanted = head == group * per_group + columns // width
    return jnp.dot(terms, wanted.astype(f32).astype(bf16), preferred_element_type=f32)


def convolved(own_ref, before_ref, after_ref, weight_ref, scratch):
    tokens = own_ref.shape[0]
    scratch[pl.ds(SUBLANES, tokens)] = own_ref[...].astype(f32)
    scratch[pl.ds(SUBLANES - HALF, HALF)] = before_ref[...].astype(f32)
    scratch[pl.ds(SUBLANES + tokens, HALF)] = after_ref[...].astype(f32)
    weights = weight_ref[...].astype(f32)
    total = weights[0:1] * scratch[pl.ds(SUBLANES - HALF, tokens)]
    for o in range(1, TAPS):
        total = total + weights[o : o + 1] * scratch[pl.ds(SUBLANES - HALF + o, tokens)]
    return total


def silu(x):
    return x / (1.0 + jnp.exp(-x))


def local_kernel(
    value_ref,
    value_before,
    value_after,
    value_weight,
    key_ref,
    key_before,
    key_after,
    key_weight,
    query_ref,
    query_before,
    query_after,
    query_weight,
    column_terms,
    row_terms,
    state_terms,
    extra_ref,
    inner_ref,
    query_out,
    sent_ref,
    wide,
    narrow,
    *,
    heads,
    per_group,
    columns,
):
    group = pl.program_id(0)
    tokens = value_ref.shape[0]
    width = value_ref.shape[1]
    values = convolved(value_ref, value_before, value_after, value_weight, wide).astype(bf16)
    keys = silu(convolved(key_ref, key_before, key_after, key_weight, narrow)).astype(bf16)
    queries = silu(convolved(query_ref, query_before, query_after, query_weight, narrow))
    queries = queries.astype(bf16)
    query_out[...] = queries
    scores = lax.dot_general(
        queries, keys, (((1,), (1,)), ((), ())), preferred_element_type=f32
    )
    row = lax.broadcasted_iota(jnp.int32, (tokens, tokens), 0)
    column = lax.broadcasted_iota(jnp.int32, (tokens, tokens), 1)
    below, above = row > column, row < column
    forward_columns = pick_heads(column_terms[0], heads, group, per_group, LANES, 3)
    backward_columns = pick_heads(column_terms[1], heads, group, per_group, LANES, 3)
    for j in range(per_group):
        lanes = slice(j * LANES, (j + 1) * LANES)
        spread = [forward_columns[:, lanes]] * (tokens // LANES)
        forward = jnp.concatenate(spread, axis=1) - row_terms[0, 0, j : j + 1]
        spread = [backward_columns[:, lanes]] * (tokens // LANES)
        backward = row_terms[1, 0, j : j + 1] - jnp.concatenate(spread, axis=1)
        both = jnp.broadcast_to(row_terms[2, 0, j : j + 1], (tokens, tokens))
        exponent = jnp.where(below, forward, jnp.where(above, backward, both))
        weight = (scores * jnp.exp(exponent)).astype(bf16)
        part = slice(j * HEAD_DIM, (j + 1) * HEAD_DIM)
        inner_ref[:, part] = jnp.dot(weight, values[:, part], preferred_element_type=f32)
    for d in range(2):
        factor = pick_heads(state_terms[d], heads, group, per_group, HEAD_DIM, 2)
        scaled = (values.astype(f32) * factor).astype(bf16)
        state = lax.dot_general(
            keys, scaled, (((0,), (0,)), ((), ())), preferred_element_type=f32
        )
        start = pl.multiple_of(d * columns + group * width, LANES)
        sent_ref[:, pl.ds(start, width)] = state.astype(bf16)

    @pl.when(group == 0)
    def _():
        sent_ref[:, 2 * columns :] = jnp.broadcast_to(
            extra_ref[...], (sent_ref.shape[0], extra_ref.shape[1])
        )


def carry_kernel(arrived_ref, answer_ref, *, heads, columns):
    count = arrived_ref.shape[0]
    lanes = arrived_ref.shape[2] - 2 * columns
    extra = jnp.concatenate(
        [arrived_ref[k, 0:1, 2 * columns :].astype(f32) for k in range(count)], axis=0
    ).astype(bf16)
    index = lax.broadcasted_iota(jnp.int32, (lanes, 2 * columns), 0)
    column = lax.broadcasted_iota(jnp.int32, (lanes, 2 * columns), 1)
    head = jnp.where(index >= 2 * heads, index - 2 * heads, index)
    wanted = (head == column // (columns // heads)) & (index < 4 * heads)
    decays = jnp.dot(extra, wanted.astype(f32).astype(bf16), preferred_element_type=f32)
    forward = slice(0, columns)
    backward = slice(columns, 2 * columns)
    carried = jnp.zeros((arrived_ref.shape[1], columns), f32)
    for k in range(count):
        answer_ref[k, :, forward] = carried.astype(bf16)
        carried = carried * decays[k : k + 1, forward] + arrived_ref[k, :, forward].astype(f32)
    carried = jnp.zeros((arrived_ref.shape[1], columns), f32)
    for k in reversed(range(count)):
        answer_ref[k, :, backward] = carried.astype(bf16)
        carried = carried * decays[k : k + 1, backward] + arrived_ref[k, :, backward].astype(f32)


def output_kernel(
    position_ref,
    query_ref,
    entering_ref,
    leaving_ref,
    inner_ref,
    gate_ref,
    read_terms,
    gain_ref,
    *rest,
    heads,
    per_group,
    count,
):
    matrices, out_ref, total = rest[:count], rest[count], rest[count + 1]
    group = pl.program_id(0)
    tokens, width = inner_ref.shape
    me = position_ref[0]
    queries = query_ref[...]
    mixed = inner_ref[...]
    for d, states in ((0, entering_ref), (1, leaving_ref)):
        factor = pick_heads(read_terms[d], heads, group, per_group, HEAD_DIM, 2)
        mixed = mixed + factor * jnp.dot(queries, states[...], preferred_element_type=f32)
    gated = mixed * silu(gate_ref[...].astype(f32))
    squares = gated * gated
    high = squares.astype(bf16)
    low = (squares - high.astype(f32)).astype(bf16)
    row = lax.broadcasted_iota(jnp.int32, (width, width), 0)
    column = lax.broadcasted_iota(jnp.int32, (width, width), 1)
    same = (row // HEAD_DIM == column // HEAD_DIM).astype(f32).astype(bf16)
    mean = jnp.dot(high, same, preferred_element_type=f32)
    mean = (mean + jnp.dot(low, same, preferred_element_type=f32)) * (1.0 / HEAD_DIM)
    normed = (gated * lax.rsqrt(mean + epsilon) * gain_ref[...]).astype(bf16)
    products = [jnp.dot(normed, m[...], preferred_element_type=f32) for m in matrices]
    block = matrices[0].shape[1]

    @pl.when(group == 0)
    def _():
        for t in range(count):
            total[t] = products[t]

    @pl.when(group > 0)
    def _():
        for t in range(count):
            total[t] += products[t]

    @pl.when(group == pl.num_programs(0) - 1)
    def _():
        rows = tokens // count
        for p, r in enumerate(butterfly_order(count)):
            first = pl.multiple_of((me ^ r) * rows, SUBLANES)
            for t in range(count):
                start = pl.multiple_of((me ^ t) * block, LANES)
                out_ref[p, :, pl.ds(start, block)] = total[t, pl.ds(first, rows), :].astype(bf16)


def expert_kernel(rows_ref, gate_ref, up_ref, down_ref, out_ref):
    rows = rows_ref[...]
    hidden = gate_ref.shape[2]
    tile = min(256, hidden)
    total = None
    for f in range(hidden // tile):
        part = slice(f * tile, (f + 1) * tile)
        gate = jnp.dot(rows, gate_ref[0, :, part], preferred_element_type=f32)
        up = jnp.dot(rows, up_ref[0, :, part], preferred_element_type=f32)
        product = jnp.dot(
            (silu(gate) * up).astype(bf16), down_ref[0, part, :], preferred_element_type=f32
        )
        total = product if total is None else total + product
    out_ref[...] = total.astype(bf16)


def expert_rows(rows, gate_matrix, up_matrix, down_matrix):
    count, width = rows.shape
    hidden = gate_matrix.shape[2]
    return pl.pallas_call(
        expert_kernel,
        name="expert_rows",
        in_specs=[pl.BlockSpec(memory_space=pltpu.VMEM)] * 4,
        out_specs=pl.BlockSpec(memory_space=pltpu.VMEM),
        out_shape=jax.ShapeDtypeStruct((count, width), bf16),
        cost_estimate=pl.CostEstimate(
            flops=6 * count * width * hidden,
            transcendentals=count * hidden,
            bytes_accessed=6 * width * hidden + 4 * count * width,
        ),
        compiler_params=pltpu.CompilerParams(vmem_limit_bytes=30 << 20),
    )(rows, gate_matrix, up_matrix, down_matrix)


def mix_tokens(
    value_projected,
    key_projected,
    query_projected,
    output_gate_projected,
    step_projected_raw,
    head_decay_logarithm,
    position_extra_decay,
    value_filter_weight,
    key_filter_weight,
    query_filter_weight,
    head_norm_gain,
    own_columns,
):
    tokens, columns = value_projected.shape
    key_width = key_projected.shape[1]
    heads = step_projected_raw.shape[2]
    groups = key_width // STATE
    per_group = heads // groups
    width = per_group * HEAD_DIM
    experts = lax.axis_size("sp")
    count = lax.axis_size("tp")
    before, after = halo_rows([value_projected, key_projected, query_projected])
    steps = jax.nn.softplus(step_projected_raw.astype(f32))
    decay = -jnp.exp(head_decay_logarithm)[:, None, :] * steps + position_extra_decay[None]
    running = jnp.einsum("ls,dsh->dlh", prefix_matrix(tokens), decay, precision=highest)
    forward = running[0]
    backward = running[1] - decay[1]
    totals = running[:, tokens - 1]
    log_steps = jnp.log(steps)
    column_terms = jnp.stack([parts_of(forward, 3), parts_of(backward, 3)])
    row_terms = jnp.stack(
        [
            (forward - log_steps[0]).T,
            (backward + log_steps[1]).T,
            jnp.log(steps[0] + steps[1]).T,
        ]
    ).reshape(3, groups, per_group, tokens)
    state_terms = jnp.stack(
        [
            parts_of(jnp.exp(totals[0] - forward) * steps[0], 2),
            parts_of(jnp.exp(backward) * steps[1], 2),
        ]
    )
    read_terms = jnp.stack(
        [parts_of(jnp.exp(forward), 2), parts_of(jnp.exp(totals[1] - backward), 2)]
    )
    extra = parts_of(jnp.exp(totals).reshape(1, 2 * heads), 2)
    extra_lanes = -(-extra.shape[1] // LANES) * LANES
    extra = jnp.pad(extra, ((0, 0), (0, extra_lanes - extra.shape[1])))
    value_blocks, key_blocks = columns // STATE, key_width // STATE

    def whole(x):
        return pl.BlockSpec(x.shape, lambda g: (0,) * x.ndim)

    def columns_of(rows, size, offset):
        return pl.BlockSpec((rows, size), lambda g: (0, offset + g))

    inner, queries, sent = pl.pallas_call(
        functools.partial(local_kernel, heads=heads, per_group=per_group, columns=columns),
        name="local_mix",
        grid=(groups,),
        in_specs=[
            columns_of(tokens, width, 0),
            columns_of(HALF, width, 0),
            columns_of(HALF, width, 0),
            columns_of(TAPS, width, 0),
            columns_of(tokens, STATE, 0),
            columns_of(HALF, STATE, value_blocks),
            columns_of(HALF, STATE, value_blocks),
            columns_of(TAPS, STATE, 0),
            columns_of(tokens, STATE, 0),
            columns_of(HALF, STATE, value_blocks + key_blocks),
            columns_of(HALF, STATE, value_blocks + key_blocks),
            columns_of(TAPS, STATE, 0),
            whole(column_terms),
            pl.BlockSpec((3, 1, per_group, tokens), lambda g: (0, g, 0, 0)),
            whole(state_terms),
            whole(extra),
        ],
        out_specs=[
            columns_of(tokens, width, 0),
            columns_of(tokens, STATE, 0),
            pl.BlockSpec((STATE, 2 * columns + extra_lanes), lambda g: (0, 0)),
        ],
        out_shape=[
            jax.ShapeDtypeStruct((tokens, columns), f32),
            jax.ShapeDtypeStruct((tokens, key_width), bf16),
            jax.ShapeDtypeStruct((STATE, 2 * columns + extra_lanes), bf16),
        ],
        scratch_shapes=[
            pltpu.VMEM((tokens + 2 * SUBLANES, width), f32),
            pltpu.VMEM((tokens + 2 * SUBLANES, STATE), f32),
        ],
        compiler_params=pltpu.CompilerParams(
            dimension_semantics=("arbitrary",), vmem_limit_bytes=60 << 20
        ),
    )(
        value_projected,
        before,
        after,
        value_filter_weight,
        key_projected,
        before,
        after,
        key_filter_weight,
        query_projected,
        before,
        after,
        query_filter_weight,
        column_terms,
        row_terms,
        state_terms,
        extra,
    )
    sent = sent.reshape(experts, STATE // experts, sent.shape[1])
    arrived = lax.all_to_all(sent, "sp", split_axis=0, concat_axis=0, tiled=True)
    answer = pl.pallas_call(
        functools.partial(carry_kernel, heads=heads, columns=columns),
        name="carry",
        out_shape=jax.ShapeDtypeStruct((experts, STATE // experts, 2 * columns), bf16),
        compiler_params=pltpu.CompilerParams(vmem_limit_bytes=60 << 20),
    )(arrived)
    states = lax.all_to_all(answer, "sp", split_axis=0, concat_axis=0, tiled=True)
    states = states.reshape(STATE, 2 * columns)
    block = own_columns[0].shape[1]
    position = lax.axis_index("tp").astype(jnp.int32).reshape(1)
    gain = head_norm_gain.reshape(1, columns)
    return pl.pallas_call(
        functools.partial(output_kernel, heads=heads, per_group=per_group, count=count),
        name="mix_output",
        grid=(groups,),
        in_specs=[
            pl.BlockSpec(memory_space=pltpu.SMEM),
            columns_of(tokens, STATE, 0),
            columns_of(STATE, width, 0),
            columns_of(STATE, width, groups),
            columns_of(tokens, width, 0),
            columns_of(tokens, width, 0),
            whole(read_terms),
            columns_of(1, width, 0),
        ]
        + [pl.BlockSpec((width, block), lambda g: (g, 0)) for _ in own_columns],
        out_specs=pl.BlockSpec((count, tokens // count, count * block), lambda g: (0, 0, 0)),
        out_shape=jax.ShapeDtypeStruct((count, tokens // count, count * block), bf16),
        scratch_shapes=[pltpu.VMEM((count, tokens, block), f32)],
        compiler_params=pltpu.CompilerParams(
            dimension_semantics=("arbitrary",), vmem_limit_bytes=60 << 20
        ),
    )(
        position,
        queries,
        states,
        states,
        inner,
        output_gate_projected,
        read_terms,
        gain,
        *own_columns,
    )


def slot_table(route_rows, experts, capacity, here):
    flat_ids = route_rows.reshape(-1)
    expert_ids = lax.broadcasted_iota(jnp.int32, (flat_ids.shape[0], experts), 1)
    matches = (flat_ids[:, None] == expert_ids).astype(f32)
    below = prefix_matrix(flat_ids.shape[0]).astype(bf16)
    running = jnp.dot(below, matches.astype(bf16), preferred_element_type=f32)
    rank_in = (jnp.sum(matches * running, axis=1) - 1.0).astype(jnp.int32)
    return ((flat_ids ^ here) * capacity + rank_in).reshape(route_rows.shape)


def own_row_blocks(matrix, rows):
    me = lax.axis_index("tp")
    parts = []
    for t in range(lax.axis_size("tp")):
        block = lax.dynamic_slice_in_dim(matrix, (me ^ t) * rows, rows, 0)
        parts.append(exchange(block, "tp", t) if t else block)
    return parts


def chunks_of(experts):
    quarter = max(experts // 4, 1)
    return [range(0, 2 * quarter), range(2 * quarter, 3 * quarter), range(3 * quarter, experts)]


def shards(
    residual_layer_input,
    value_projected,
    key_projected,
    query_projected,
    output_gate_projected,
    step_projected_raw,
    head_decay_logarithm,
    position_extra_decay,
    value_filter_weight,
    key_filter_weight,
    query_filter_weight,
    head_norm_gain,
    mixer_output_matrix,
    expert_norm_gain,
    routes,
    chosen_expert_weight,
    expert_gate_matrix,
    expert_up_matrix,
    expert_down_matrix,
):
    experts = lax.axis_size("sp")
    here = lax.axis_index("sp")
    position = lax.axis_index("tp")
    own_rows, model_width = residual_layer_input.shape
    top_count = routes.shape[1]
    capacity = 2 * own_rows * top_count // experts
    places = experts * capacity
    own_columns = own_row_blocks(mixer_output_matrix, value_projected.shape[1])
    own_routes = lax.dynamic_slice_in_dim(routes, position * own_rows, own_rows, 0)
    own_slots = slot_table(own_routes, experts, capacity, here)
    place_ids = lax.broadcasted_iota(jnp.int32, (places,) + own_slots.shape, 0)
    one_hot = jnp.sum((place_ids == own_slots[None]).astype(f32), axis=2).astype(bf16)
    chosen = (
        lax.broadcasted_iota(jnp.int32, (own_rows, top_count, places), 2) == own_slots[:, :, None]
    )
    mixing = jnp.sum(jnp.where(chosen, chosen_expert_weight[:, :, None], 0.0), axis=1)
    mixing_high = mixing.astype(bf16)
    mixing_low = (mixing - mixing_high.astype(f32)).astype(bf16)

    partial = mix_tokens(
        value_projected,
        key_projected,
        query_projected,
        output_gate_projected,
        step_projected_raw,
        head_decay_logarithm,
        position_extra_decay,
        value_filter_weight,
        key_filter_weight,
        query_filter_weight,
        head_norm_gain,
        own_columns,
    )
    mixer_out = scatter_rows(partial, "tp")
    middle = add_rounded(residual_layer_input, mixer_out)
    residual = middle.astype(f32)
    normed = (
        residual
        * lax.rsqrt(jnp.mean(residual * residual, axis=-1, keepdims=True) + epsilon)
        * expert_norm_gain
    ).astype(bf16)
    outgoing = jnp.dot(one_hot, normed, preferred_element_type=f32).astype(bf16)
    outgoing = outgoing.reshape(experts, capacity, model_width)
    returned = []
    for chunk in chunks_of(experts):
        arrived = [exchange(outgoing[d], "sp", d) if d else outgoing[d] for d in chunk]
        blocks = gather_rows(jnp.concatenate(arrived, axis=0), "tp")
        partial_sum = expert_rows(
            blocks.reshape(-1, model_width),
            expert_gate_matrix,
            expert_up_matrix,
            expert_down_matrix,
        )
        summed = scatter_rows(partial_sum.reshape(blocks.shape), "tp")
        results = summed.reshape(len(chunk), capacity, model_width)
        returned += [
            exchange(results[i], "sp", d) if d else results[i] for i, d in enumerate(chunk)
        ]
    returned = jnp.concatenate(returned, axis=0)
    expert_mix = jnp.dot(mixing_high, returned, preferred_element_type=f32)
    expert_mix = expert_mix + jnp.dot(mixing_low, returned, preferred_element_type=f32)
    return (residual + expert_mix).astype(bf16)


def solution(mesh):
    return jax.shard_map(
        shards,
        mesh=mesh,
        in_specs=(
            P(("sp", "tp"), None),
            P("sp", "tp"),
            P("sp", "tp"),
            P("sp", "tp"),
            P("sp", "tp"),
            P(None, "sp", "tp"),
            P(None, "tp"),
            P("sp", "tp"),
            P(None, "tp"),
            P(None, "tp"),
            P(None, "tp"),
            P("tp"),
            P(None, "tp"),
            P(),
            P("sp", None),
            P(("sp", "tp"), None),
            P("sp", None, "tp"),
            P("sp", None, "tp"),
            P("sp", "tp", None),
        ),
        out_specs=P(("sp", "tp"), None),
        check_vma=False,
    )
```

```python
import functools

import jax
import jax.numpy as jnp
from jax import lax
from jax.experimental import pallas as pl
from jax.experimental.pallas import tpu as pltpu
from jax.sharding import PartitionSpec as P


HEAD_DIM = 64
STATE = 128
TAPS = 5
HALF = (TAPS - 1) // 2
LANES = 128
SUBLANES = 8
MIX_BYTES = 57 << 20

epsilon = 1e-06
highest = lax.Precision.HIGHEST
f32 = jnp.float32
bf16 = jnp.bfloat16


def exchange(x, axis, distance):
    count = lax.axis_size(axis)
    return lax.ppermute(x, axis, [(i, i ^ distance) for i in range(count)])


def bits_of(count):
    return [1 << k for k in range(count.bit_length() - 1)]


def butterfly_order(count):
    order = [0]
    for bit in reversed(bits_of(count)):
        order = order + [b ^ bit for b in order]
    return order


def joined(blocks):
    return blocks[0] if len(blocks) == 1 else jnp.concatenate(blocks, axis=0)


def gather_rows(rows, axis):
    parts = [rows]
    for bit in reversed(bits_of(lax.axis_size(axis))):
        sent = joined(parts)
        parts.append(exchange(sent, axis, bit))
    return parts


def add_rounded(a, b):
    return (a.astype(f32) + b.astype(f32)).astype(bf16)


def scatter_rows(kept, sent, axis):
    for bit in bits_of(lax.axis_size(axis)):
        received = exchange(sent, axis, bit)
        if 2 * bit == lax.axis_size(axis):
            return add_rounded(kept, received)
        half = kept.shape[0] // 2
        kept, sent = (
            add_rounded(kept[:half], received[:half]),
            add_rounded(kept[half:], received[half:]),
        )


def prefix_matrix(length):
    row_index = lax.broadcasted_iota(jnp.int32, (length, length), 0)
    column_index = lax.broadcasted_iota(jnp.int32, (length, length), 1)
    return (column_index <= row_index).astype(f32)


def halo_rows(parts):
    count = lax.axis_size("sp")
    pairs = [(i, i + 1) for i in range(count - 1)]
    tail = jnp.concatenate([p[p.shape[0] - HALF :] for p in parts], axis=1)
    head = jnp.concatenate([p[:HALF] for p in parts], axis=1)
    before = lax.ppermute(tail, "sp", pairs)
    after = lax.ppermute(head, "sp", [(b, a) for a, b in pairs])
    return before, after


def pick_heads(terms, heads, group, per_group, width):
    shape = (terms.shape[0], per_group * width)
    head = lax.broadcasted_iota(jnp.int32, shape, 0) % heads
    columns = lax.broadcasted_iota(jnp.int32, shape, 1)
    wanted = (head == group * per_group + columns // width).astype(f32).astype(bf16)
    return lax.dot_general(
        terms, wanted, (((0,), (0,)), ((), ())), preferred_element_type=f32
    )


def convolved(own_ref, before_ref, after_ref, weight_ref, scratch):
    tokens = own_ref.shape[0]
    scratch[pl.ds(SUBLANES, tokens)] = own_ref[...].astype(f32)
    scratch[pl.ds(SUBLANES - HALF, HALF)] = before_ref[...].astype(f32)
    scratch[pl.ds(SUBLANES + tokens, HALF)] = after_ref[...].astype(f32)
    weights = weight_ref[...].astype(f32)
    total = weights[0:1] * scratch[pl.ds(SUBLANES - HALF, tokens)]
    for o in range(1, TAPS):
        total = total + weights[o : o + 1] * scratch[pl.ds(SUBLANES - HALF + o, tokens)]
    return total


def silu(x):
    return x / (1.0 + jnp.exp(-x))


def decay_kernel(raw_ref, rate_ref, position_ref, *outs):
    tokens = raw_ref.shape[2]
    row = lax.broadcasted_iota(jnp.int32, (tokens, tokens), 0)
    column = lax.broadcasted_iota(jnp.int32, (tokens, tokens), 1)
    prefix = (row <= column).astype(f32)
    heads = raw_ref.shape[1]
    row = lax.broadcasted_iota(jnp.int32, (heads, heads), 0)
    own = row == lax.broadcasted_iota(jnp.int32, (heads, heads), 1)
    steps, decays, sums = [], [], []
    for d in range(2):
        raw = raw_ref[d].astype(f32)
        steps.append(jnp.maximum(raw, 0.0) + jnp.log1p(jnp.exp(-jnp.abs(raw))))
        rate = jnp.sum(jnp.where(own, jnp.exp(rate_ref[d : d + 1]), 0.0), axis=1, keepdims=True)
        decays.append(position_ref[...] - rate * steps[d])
        sums.append(
            jnp.dot(decays[d], prefix, precision=highest, preferred_element_type=f32)
        )
    forward, backward = sums[0], sums[1] - decays[1]
    forward_total, backward_total = sums[0][:, tokens - 1 :], sums[1][:, tokens - 1 :]
    terms = (
        forward,
        backward,
        jnp.exp(forward_total - forward) * steps[0],
        jnp.exp(backward) * steps[1],
        jnp.exp(forward),
        jnp.exp(backward_total - backward),
    )
    for ref, x in zip(outs, terms):
        for k in range(ref.shape[0]):
            part = x.astype(bf16)
            ref[k] = part
            x = x - part.astype(f32)
    outs[6][...] = forward - jnp.log(steps[0])
    outs[7][...] = backward + jnp.log(steps[1])
    outs[8][...] = jnp.log(steps[0] + steps[1])
    outs[9][...] = jnp.zeros(outs[9].shape, f32)
    for d, total in enumerate((forward_total, backward_total)):
        flat = jnp.sum(jnp.where(own, jnp.exp(total), 0.0), axis=0, keepdims=True)
        high = flat.astype(bf16).astype(f32)
        outs[9][:, d * heads : (d + 1) * heads] = high
        outs[9][:, (2 + d) * heads : (3 + d) * heads] = flat - high


def local_kernel(
    value_ref,
    value_before,
    value_after,
    value_weight,
    key_ref,
    key_before,
    key_after,
    key_weight,
    forward_terms,
    backward_terms,
    extra_ref,
    value_out,
    key_out,
    sent_ref,
    wide,
    narrow,
    *,
    heads,
    per_group,
    columns,
):
    group = pl.program_id(0)
    width = value_ref.shape[1]
    values = convolved(value_ref, value_before, value_after, value_weight, wide).astype(bf16)
    value_out[...] = values
    keys = silu(convolved(key_ref, key_before, key_after, key_weight, narrow)).astype(bf16)
    key_out[...] = keys
    for d, terms in ((0, forward_terms), (1, backward_terms)):
        factor = pick_heads(terms[...], heads, group, per_group, HEAD_DIM)
        scaled = (values.astype(f32) * factor).astype(bf16)
        state = lax.dot_general(
            keys, scaled, (((0,), (0,)), ((), ())), preferred_element_type=f32
        )
        start = pl.multiple_of(d * columns + group * width, LANES)
        sent_ref[:, pl.ds(start, width)] = state.astype(bf16)

    @pl.when(group == 0)
    def _():
        sent_ref[:, 2 * columns :] = jnp.broadcast_to(
            extra_ref[...].astype(bf16), (sent_ref.shape[0], extra_ref.shape[1])
        )


def inner_kernel(
    value_ref,
    key_ref,
    query_ref,
    query_before,
    query_after,
    query_weight,
    forward_terms,
    backward_terms,
    forward_row,
    backward_row,
    both_row,
    inner_ref,
    query_out,
    narrow,
    *,
    heads,
    per_group,
):
    group = pl.program_id(0)
    tokens = value_ref.shape[0]
    values = value_ref[...]
    queries = silu(convolved(query_ref, query_before, query_after, query_weight, narrow))
    queries = queries.astype(bf16)
    query_out[...] = queries
    scores = lax.dot_general(
        queries, key_ref[...], (((1,), (1,)), ((), ())), preferred_element_type=f32
    )
    row = lax.broadcasted_iota(jnp.int32, (tokens, tokens), 0)
    column = lax.broadcasted_iota(jnp.int32, (tokens, tokens), 1)
    below, above = row > column, row < column
    forward_columns = pick_heads(forward_terms[...], heads, group, per_group, LANES)
    backward_columns = pick_heads(backward_terms[...], heads, group, per_group, LANES)
    for j in range(per_group):
        lanes = slice(j * LANES, (j + 1) * LANES)
        own = pl.ds(group * per_group + j, 1)
        spread = [forward_columns[:, lanes]] * (tokens // LANES)
        forward = jnp.concatenate(spread, axis=1) - forward_row[own, :]
        spread = [backward_columns[:, lanes]] * (tokens // LANES)
        backward = backward_row[own, :] - jnp.concatenate(spread, axis=1)
        both = jnp.broadcast_to(both_row[own, :], (tokens, tokens))
        exponent = jnp.where(below, forward, jnp.where(above, backward, both))
        weight = (scores * jnp.exp(exponent)).astype(bf16)
        part = slice(j * HEAD_DIM, (j + 1) * HEAD_DIM)
        inner_ref[:, part] = jnp.dot(weight, values[:, part], preferred_element_type=f32)


def carry_kernel(arrived_ref, answer_ref, *, heads, columns):
    count = arrived_ref.shape[0]
    lanes = arrived_ref.shape[2] - 2 * columns
    extra = jnp.concatenate(
        [arrived_ref[k, 0:1, 2 * columns :].astype(f32) for k in range(count)], axis=0
    ).astype(bf16)
    index = lax.broadcasted_iota(jnp.int32, (lanes, 2 * columns), 0)
    column = lax.broadcasted_iota(jnp.int32, (lanes, 2 * columns), 1)
    head = jnp.where(index >= 2 * heads, index - 2 * heads, index)
    wanted = (head == column // (columns // heads)) & (index < 4 * heads)
    decays = jnp.dot(extra, wanted.astype(f32).astype(bf16), preferred_element_type=f32)
    forward = slice(0, columns)
    backward = slice(columns, 2 * columns)
    carried = jnp.zeros((arrived_ref.shape[1], columns), f32)
    for k in range(count):
        answer_ref[k, :, forward] = carried.astype(bf16)
        carried = carried * decays[k : k + 1, forward] + arrived_ref[k, :, forward].astype(f32)
    carried = jnp.zeros((arrived_ref.shape[1], columns), f32)
    for k in reversed(range(count)):
        answer_ref[k, :, backward] = carried.astype(bf16)
        carried = carried * decays[k : k + 1, backward] + arrived_ref[k, :, backward].astype(f32)


def output_kernel(
    position_ref,
    query_ref,
    entering_ref,
    leaving_ref,
    inner_ref,
    gate_ref,
    entering_terms,
    leaving_terms,
    gain_ref,
    *rest,
    heads,
    per_group,
    count,
):
    matrices = rest[:count]
    kept_ref, sent_ref, total = rest[-3:]
    group = pl.program_id(0)
    tokens, width = inner_ref.shape
    me = position_ref[0]
    queries = query_ref[...]
    mixed = inner_ref[...]
    for terms, states in ((entering_terms, entering_ref), (leaving_terms, leaving_ref)):
        factor = pick_heads(terms[...], heads, group, per_group, HEAD_DIM)
        mixed = mixed + factor * jnp.dot(queries, states[...], preferred_element_type=f32)
    gated = mixed * silu(gate_ref[...].astype(f32))
    squares = gated * gated
    high = squares.astype(bf16)
    low = (squares - high.astype(f32)).astype(bf16)
    row = lax.broadcasted_iota(jnp.int32, (width, width), 0)
    column = lax.broadcasted_iota(jnp.int32, (width, width), 1)
    same = (row // HEAD_DIM == column // HEAD_DIM).astype(f32).astype(bf16)
    mean = jnp.dot(high, same, preferred_element_type=f32)
    mean = (mean + jnp.dot(low, same, preferred_element_type=f32)) * (1.0 / HEAD_DIM)
    normed = (gated * lax.rsqrt(mean + epsilon) * gain_ref[...]).astype(bf16)
    products = [jnp.dot(normed, m[...], preferred_element_type=f32) for m in matrices]
    block = matrices[0].shape[1]

    @pl.when(group == 0)
    def _():
        for t in range(count):
            total[t] = products[t]

    @pl.when(group > 0)
    def _():
        for t in range(count):
            total[t] += products[t]

    @pl.when(group == pl.num_programs(0) - 1)
    def _():
        rows = tokens // count
        for p, r in enumerate(butterfly_order(count)):
            out_ref = kept_ref if 2 * p < count else sent_ref
            place = slice(p % (count // 2) * rows, (p % (count // 2) + 1) * rows)
            first = pl.multiple_of((me ^ r) * rows, SUBLANES)
            for t in range(count):
                start = pl.multiple_of((me ^ t) * block, LANES)
                out_ref[place, pl.ds(start, block)] = total[t, pl.ds(first, rows), :].astype(bf16)


def hold_kernel(*refs):
    count = len(refs) // 3
    copies = [
        pltpu.make_async_copy(refs[k], refs[count + k], refs[2 * count + k]) for k in range(count)
    ]
    for copy in copies:
        copy.start()
    for copy in copies:
        copy.wait()


def held(matrices):
    return pl.pallas_call(
        hold_kernel,
        name="hold",
        in_specs=[pl.BlockSpec(memory_space=pltpu.HBM) for _ in matrices],
        out_specs=[pl.BlockSpec(memory_space=pltpu.VMEM) for _ in matrices],
        out_shape=[jax.ShapeDtypeStruct(m.shape, m.dtype) for m in matrices],
        scratch_shapes=[pltpu.SemaphoreType.DMA for _ in matrices],
        compiler_params=pltpu.CompilerParams(vmem_limit_bytes=16 << 20),
    )(*matrices)


def expert_kernel(*refs):
    *row_refs, gate_ref, up_ref, down_ref, kept_ref, sent_ref = refs
    rows = joined([r[...] for r in row_refs])
    hidden = gate_ref.shape[2]
    tile = min(256, hidden)
    total = None
    for f in range(hidden // tile):
        part = slice(f * tile, (f + 1) * tile)
        gate = jnp.dot(rows, gate_ref[0, :, part], preferred_element_type=f32)
        up = jnp.dot(rows, up_ref[0, :, part], preferred_element_type=f32)
        product = jnp.dot(
            (silu(gate) * up).astype(bf16), down_ref[0, part, :], preferred_element_type=f32
        )
        total = product if total is None else total + product
    half = kept_ref.shape[0]
    kept_ref[...] = total[:half].astype(bf16)
    sent_ref[...] = total[half:].astype(bf16)


def expert_rows(parts, gate_matrix, up_matrix, down_matrix):
    width = parts[0].shape[1]
    count = sum(p.shape[0] for p in parts)
    hidden = gate_matrix.shape[2]
    return pl.pallas_call(
        expert_kernel,
        name="expert_rows",
        in_specs=[pl.BlockSpec(memory_space=pltpu.VMEM)] * (len(parts) + 3),
        out_specs=[pl.BlockSpec(memory_space=pltpu.VMEM)] * 2,
        out_shape=[jax.ShapeDtypeStruct((count // 2, width), bf16)] * 2,
        cost_estimate=pl.CostEstimate(
            flops=6 * count * width * hidden,
            transcendentals=count * hidden,
            bytes_accessed=6 * width * hidden + 4 * count * width,
        ),
        compiler_params=pltpu.CompilerParams(vmem_limit_bytes=30 << 20),
    )(*parts, gate_matrix, up_matrix, down_matrix)


def final_kernel(middle_ref, mixing_ref, *refs):
    *returned, out_ref = refs
    rows = joined([r[...] for r in returned])
    mixing = mixing_ref[...]
    high = mixing.astype(bf16)
    low = (mixing - high.astype(f32)).astype(bf16)
    total = jnp.dot(high, rows, preferred_element_type=f32)
    total = total + jnp.dot(low, rows, preferred_element_type=f32)
    out_ref[...] = (middle_ref[...].astype(f32) + total).astype(bf16)


def mix_tokens(
    value_projected,
    key_projected,
    query_projected,
    output_gate_projected,
    step_projected_raw,
    head_decay_logarithm,
    position_extra_decay,
    value_filter_weight,
    key_filter_weight,
    query_filter_weight,
    head_norm_gain,
    mixer_output_matrix,
):
    tokens, columns = value_projected.shape
    key_width = key_projected.shape[1]
    heads = step_projected_raw.shape[2]
    groups = key_width // STATE
    per_group = heads // groups
    width = per_group * HEAD_DIM
    experts = lax.axis_size("sp")
    count = lax.axis_size("tp")
    before, after = halo_rows([value_projected, key_projected, query_projected])
    early = own_row_block(mixer_output_matrix, columns, count // 2)
    shapes = [(3, heads, tokens)] * 2 + [(2, heads, tokens)] * 4
    shapes = [jax.ShapeDtypeStruct(k, bf16) for k in shapes]
    shapes += [jax.ShapeDtypeStruct((heads, tokens), f32)] * 3
    extra_lanes = -(-4 * heads // LANES) * LANES
    shapes += [jax.ShapeDtypeStruct((1, extra_lanes), f32)]
    outs = pl.pallas_call(
        decay_kernel,
        name="decays",
        out_shape=shapes,
        compiler_params=pltpu.CompilerParams(vmem_limit_bytes=60 * 1024 * 1024),
    )(
        jnp.swapaxes(step_projected_raw, 1, 2),
        head_decay_logarithm,
        position_extra_decay.T,
    )
    terms = [t.reshape(-1, tokens) for t in outs[:6]]
    column_terms, state_terms, read_terms = terms[:2], terms[2:4], terms[4:]
    row_terms = list(outs[6:9])
    extra = outs[9]
    value_blocks, key_blocks = columns // STATE, key_width // STATE

    def whole(x):
        return pl.BlockSpec(x.shape, lambda g: (0,) * x.ndim)

    def columns_of(rows, size, offset):
        return pl.BlockSpec((rows, size), lambda g: (0, offset + g))

    values, keys, sent = pl.pallas_call(
        functools.partial(local_kernel, heads=heads, per_group=per_group, columns=columns),
        name="local_mix",
        grid=(groups,),
        in_specs=[
            columns_of(tokens, width, 0),
            columns_of(HALF, width, 0),
            columns_of(HALF, width, 0),
            columns_of(TAPS, width, 0),
            columns_of(tokens, STATE, 0),
            columns_of(HALF, STATE, value_blocks),
            columns_of(HALF, STATE, value_blocks),
            columns_of(TAPS, STATE, 0),
            whole(state_terms[0]),
            whole(state_terms[1]),
            whole(extra),
        ],
        out_specs=[
            columns_of(tokens, width, 0),
            columns_of(tokens, STATE, 0),
            pl.BlockSpec((STATE, 2 * columns + extra_lanes), lambda g: (0, 0)),
        ],
        out_shape=[
            jax.ShapeDtypeStruct((tokens, columns), bf16),
            jax.ShapeDtypeStruct((tokens, key_width), bf16),
            jax.ShapeDtypeStruct((STATE, 2 * columns + extra_lanes), bf16),
        ],
        scratch_shapes=[
            pltpu.VMEM((tokens + 2 * SUBLANES, width), f32),
            pltpu.VMEM((tokens + 2 * SUBLANES, STATE), f32),
        ],
        compiler_params=pltpu.CompilerParams(
            dimension_semantics=("arbitrary",), vmem_limit_bytes=60 << 20
        ),
    )(
        value_projected,
        before,
        after,
        value_filter_weight,
        key_projected,
        before,
        after,
        key_filter_weight,
        *state_terms,
        extra,
    )
    later_matrix, _ = lax.optimization_barrier((mixer_output_matrix, sent))
    own_columns = [
        early if t == count // 2 else own_row_block(later_matrix, columns, t)
        for t in range(count)
    ]
    inner, queries = pl.pallas_call(
        functools.partial(inner_kernel, heads=heads, per_group=per_group),
        name="inner_mix",
        grid=(groups,),
        in_specs=[
            columns_of(tokens, width, 0),
            columns_of(tokens, STATE, 0),
            columns_of(tokens, STATE, 0),
            columns_of(HALF, STATE, value_blocks + key_blocks),
            columns_of(HALF, STATE, value_blocks + key_blocks),
            columns_of(TAPS, STATE, 0),
        ]
        + [whole(t) for t in column_terms + row_terms],
        out_specs=[columns_of(tokens, width, 0), columns_of(tokens, STATE, 0)],
        out_shape=[
            jax.ShapeDtypeStruct((tokens, columns), f32),
            jax.ShapeDtypeStruct((tokens, key_width), bf16),
        ],
        scratch_shapes=[pltpu.VMEM((tokens + 2 * SUBLANES, STATE), f32)],
        cost_estimate=pl.CostEstimate(
            flops=groups * tokens * tokens * 2 * (STATE + width),
            transcendentals=groups * per_group * tokens * tokens,
            bytes_accessed=8 * tokens * columns,
        ),
        compiler_params=pltpu.CompilerParams(
            dimension_semantics=("arbitrary",), vmem_limit_bytes=60 << 20
        ),
    )(values, keys, query_projected, before, after, query_filter_weight, *column_terms, *row_terms)
    sent = sent.reshape(experts, STATE // experts, sent.shape[1])
    arrived = lax.all_to_all(sent, "sp", split_axis=0, concat_axis=0, tiled=True)
    answer = pl.pallas_call(
        functools.partial(carry_kernel, heads=heads, columns=columns),
        name="carry",
        out_shape=jax.ShapeDtypeStruct((experts, STATE // experts, 2 * columns), bf16),
        compiler_params=pltpu.CompilerParams(vmem_limit_bytes=60 * 1024 * 1024),
    )(arrived)
    states = lax.all_to_all(answer, "sp", split_axis=0, concat_axis=0, tiled=True)
    states = states.reshape(STATE, 2 * columns)
    block = own_columns[0].shape[1]
    position = lax.axis_index("tp").astype(jnp.int32).reshape(1)
    gain = head_norm_gain.reshape(1, columns)
    return pl.pallas_call(
        functools.partial(output_kernel, heads=heads, per_group=per_group, count=count),
        name="mix_output",
        grid=(groups,),
        in_specs=[
            pl.BlockSpec(memory_space=pltpu.SMEM),
            columns_of(tokens, STATE, 0),
            columns_of(STATE, width, 0),
            columns_of(STATE, width, groups),
            columns_of(tokens, width, 0),
            columns_of(tokens, width, 0),
            whole(read_terms[0]),
            whole(read_terms[1]),
            columns_of(1, width, 0),
        ]
        + [pl.BlockSpec((width, block), lambda g: (g, 0)) for _ in own_columns],
        out_specs=[pl.BlockSpec((tokens // 2, count * block), lambda g: (0, 0))] * 2,
        out_shape=[jax.ShapeDtypeStruct((tokens // 2, count * block), bf16)] * 2,
        scratch_shapes=[pltpu.VMEM((count, tokens, block), f32)],
        compiler_params=pltpu.CompilerParams(
            dimension_semantics=("arbitrary",), vmem_limit_bytes=MIX_BYTES
        ),
    )(
        position,
        queries,
        states,
        states,
        inner,
        output_gate_projected,
        *read_terms,
        gain,
        *own_columns,
    )


def slot_table(route_rows, experts, capacity, here):
    flat_ids = route_rows.reshape(-1)
    expert_ids = lax.broadcasted_iota(jnp.int32, (flat_ids.shape[0], experts), 1)
    matches = (flat_ids[:, None] == expert_ids).astype(f32)
    below = prefix_matrix(flat_ids.shape[0]).astype(bf16)
    running = jnp.dot(below, matches.astype(bf16), preferred_element_type=f32)
    rank_in = (jnp.sum(matches * running, axis=1) - 1.0).astype(jnp.int32)
    return ((flat_ids ^ here) * capacity + rank_in).reshape(route_rows.shape)


def own_row_block(matrix, rows, distance):
    block = lax.dynamic_slice_in_dim(matrix, (lax.axis_index("tp") ^ distance) * rows, rows, 0)
    return exchange(block, "tp", distance) if distance else block


def chunks_of(experts):
    quarter = max(experts // 4, 1)
    return [range(k, k + quarter) for k in range(0, experts, quarter)]


def shards(
    residual_layer_input,
    value_projected,
    key_projected,
    query_projected,
    output_gate_projected,
    step_projected_raw,
    head_decay_logarithm,
    position_extra_decay,
    value_filter_weight,
    key_filter_weight,
    query_filter_weight,
    head_norm_gain,
    mixer_output_matrix,
    expert_norm_gain,
    routes,
    chosen_expert_weight,
    expert_gate_matrix,
    expert_up_matrix,
    expert_down_matrix,
):
    experts = lax.axis_size("sp")
    here = lax.axis_index("sp")
    position = lax.axis_index("tp")
    own_rows, model_width = residual_layer_input.shape
    top_count = routes.shape[1]
    capacity = 2 * own_rows * top_count // experts
    places = experts * capacity
    own_routes = lax.dynamic_slice_in_dim(routes, position * own_rows, own_rows, 0)
    own_slots = slot_table(own_routes, experts, capacity, here)
    place_ids = lax.broadcasted_iota(jnp.int32, (places,) + own_slots.shape, 0)
    one_hot = jnp.sum((place_ids == own_slots[None]).astype(f32), axis=2).astype(bf16)
    chosen = (
        lax.broadcasted_iota(jnp.int32, (own_rows, top_count, places), 2) == own_slots[:, :, None]
    )
    mixing = jnp.sum(jnp.where(chosen, chosen_expert_weight[:, :, None], 0.0), axis=1)

    kept, sent = mix_tokens(
        value_projected,
        key_projected,
        query_projected,
        output_gate_projected,
        step_projected_raw,
        head_decay_logarithm,
        position_extra_decay,
        value_filter_weight,
        key_filter_weight,
        query_filter_weight,
        head_norm_gain,
        mixer_output_matrix,
    )
    mixer_out = scatter_rows(kept, sent, "tp")
    middle = add_rounded(residual_layer_input, mixer_out)
    residual = middle.astype(f32)
    normed = (
        residual
        * lax.rsqrt(jnp.mean(residual * residual, axis=-1, keepdims=True) + epsilon)
        * expert_norm_gain
    ).astype(bf16)
    outgoing = jnp.dot(one_hot, normed, preferred_element_type=f32).astype(bf16)
    outgoing = outgoing.reshape(experts, capacity, model_width)
    matrices = held([expert_gate_matrix, expert_up_matrix, expert_down_matrix])
    returned = []
    for chunk in chunks_of(experts):
        arrived = [exchange(outgoing[d], "sp", d) if d else outgoing[d] for d in chunk]
        parts = gather_rows(joined(arrived), "tp")
        halves = expert_rows(parts, *matrices)
        summed = scatter_rows(*halves, "tp")
        results = summed.reshape(len(chunk), capacity, model_width)
        returned += [
            exchange(results[i], "sp", d) if d else results[i] for i, d in enumerate(chunk)
        ]
    if capacity % (2 * SUBLANES):
        returned = [jnp.concatenate(returned, axis=0)]
    return pl.pallas_call(
        final_kernel,
        name="final_mix",
        out_shape=jax.ShapeDtypeStruct(middle.shape, bf16),
        compiler_params=pltpu.CompilerParams(vmem_limit_bytes=16 << 20),
    )(middle, mixing, *returned)


def solution(mesh):
    return jax.shard_map(
        shards,
        mesh=mesh,
        in_specs=(
            P(("sp", "tp"), None),
            P("sp", "tp"),
            P("sp", "tp"),
            P("sp", "tp"),
            P("sp", "tp"),
            P(None, "sp", "tp"),
            P(None, "tp"),
            P("sp", "tp"),
            P(None, "tp"),
            P(None, "tp"),
            P(None, "tp"),
            P("tp"),
            P(None, "tp"),
            P(),
            P("sp", None),
            P(("sp", "tp"), None),
            P("sp", None, "tp"),
            P("sp", None, "tp"),
            P("sp", "tp", None),
        ),
        out_specs=P(("sp", "tp"), None),
        check_vma=False,
    )
```

```python
import functools

import jax
import jax.numpy as jnp
from jax import lax
from jax.experimental import pallas as pl
from jax.experimental.pallas import tpu as pltpu
from jax.sharding import PartitionSpec as P


HEAD_DIM = 64
STATE = 128
TAPS = 5
HALF = (TAPS - 1) // 2
LANES = 128
SUBLANES = 8
MIX_BYTES = 57 << 20

epsilon = 1e-06
highest = lax.Precision.HIGHEST
f32 = jnp.float32
bf16 = jnp.bfloat16


def exchange(x, axis, distance):
    count = lax.axis_size(axis)
    return lax.ppermute(x, axis, [(i, i ^ distance) for i in range(count)])


def bits_of(count):
    return [1 << k for k in range(count.bit_length() - 1)]


def butterfly_order(count):
    order = [0]
    for bit in reversed(bits_of(count)):
        order = order + [b ^ bit for b in order]
    return order


def joined(blocks):
    return blocks[0] if len(blocks) == 1 else jnp.concatenate(blocks, axis=0)


def gather_rows(rows, axis):
    parts = [rows]
    for bit in reversed(bits_of(lax.axis_size(axis))):
        sent = joined(parts)
        parts.append(exchange(sent, axis, bit))
    return parts


def add_rounded(a, b):
    return (a.astype(f32) + b.astype(f32)).astype(bf16)


def scatter_rows(kept, sent, axis):
    for bit in bits_of(lax.axis_size(axis)):
        received = exchange(sent, axis, bit)
        if 2 * bit == lax.axis_size(axis):
            return add_rounded(kept, received)
        half = kept.shape[0] // 2
        kept, sent = (
            add_rounded(kept[:half], received[:half]),
            add_rounded(kept[half:], received[half:]),
        )


def prefix_matrix(length):
    row_index = lax.broadcasted_iota(jnp.int32, (length, length), 0)
    column_index = lax.broadcasted_iota(jnp.int32, (length, length), 1)
    return (column_index <= row_index).astype(f32)


def halo_rows(parts):
    count = lax.axis_size("sp")
    pairs = [(i, i + 1) for i in range(count - 1)]
    tail = jnp.concatenate([p[p.shape[0] - HALF :] for p in parts], axis=1)
    head = jnp.concatenate([p[:HALF] for p in parts], axis=1)
    before = lax.ppermute(tail, "sp", pairs)
    after = lax.ppermute(head, "sp", [(b, a) for a, b in pairs])
    return before, after


def halved(x, size):
    return lax.shift_right_logical(x, jnp.full(x.shape, size.bit_length() - 1, jnp.int32))


def pick_heads(terms, heads, group, per_group, width):
    shape = (terms.shape[0], per_group * width)
    head = lax.broadcasted_iota(jnp.int32, shape, 0) & (heads - 1)
    columns = lax.broadcasted_iota(jnp.int32, shape, 1)
    wanted = (head == group * per_group + halved(columns, width)).astype(f32).astype(bf16)
    return lax.dot_general(
        terms, wanted, (((0,), (0,)), ((), ())), preferred_element_type=f32
    )


def convolved(own_ref, before_ref, after_ref, weight_ref, scratch):
    tokens = own_ref.shape[0]
    scratch[pl.ds(SUBLANES, tokens)] = own_ref[...].astype(f32)
    scratch[pl.ds(SUBLANES - HALF, HALF)] = before_ref[...].astype(f32)
    scratch[pl.ds(SUBLANES + tokens, HALF)] = after_ref[...].astype(f32)
    weights = weight_ref[...].astype(f32)
    total = weights[0:1] * scratch[pl.ds(SUBLANES - HALF, tokens)]
    for o in range(1, TAPS):
        total = total + weights[o : o + 1] * scratch[pl.ds(SUBLANES - HALF + o, tokens)]
    return total


def silu(x):
    return x / (1.0 + jnp.exp(-x))


def decay_kernel(raw_ref, rate_ref, position_ref, *outs):
    tokens = raw_ref.shape[2]
    row = lax.broadcasted_iota(jnp.int32, (tokens, tokens), 0)
    column = lax.broadcasted_iota(jnp.int32, (tokens, tokens), 1)
    prefix = (row <= column).astype(f32)
    heads = raw_ref.shape[1]
    row = lax.broadcasted_iota(jnp.int32, (heads, heads), 0)
    own = row == lax.broadcasted_iota(jnp.int32, (heads, heads), 1)
    steps, decays, sums = [], [], []
    for d in range(2):
        raw = raw_ref[d].astype(f32)
        steps.append(jnp.maximum(raw, 0.0) + jnp.log1p(jnp.exp(-jnp.abs(raw))))
        rate = jnp.sum(jnp.where(own, jnp.exp(rate_ref[d : d + 1]), 0.0), axis=1, keepdims=True)
        decays.append(position_ref[...] - rate * steps[d])
        sums.append(
            jnp.dot(decays[d], prefix, precision=highest, preferred_element_type=f32)
        )
    forward, backward = sums[0], sums[1] - decays[1]
    forward_total, backward_total = sums[0][:, tokens - 1 :], sums[1][:, tokens - 1 :]
    terms = (
        forward,
        backward,
        jnp.exp(forward_total - forward) * steps[0],
        jnp.exp(backward) * steps[1],
        jnp.exp(forward),
        jnp.exp(backward_total - backward),
    )
    for ref, x in zip(outs, terms):
        for k in range(ref.shape[0]):
            part = x.astype(bf16)
            ref[k] = part
            x = x - part.astype(f32)
    outs[6][...] = forward - jnp.log(steps[0])
    outs[7][...] = backward + jnp.log(steps[1])
    outs[8][...] = jnp.log(steps[0] + steps[1])
    outs[9][...] = jnp.zeros(outs[9].shape, f32)
    for d, total in enumerate((forward_total, backward_total)):
        flat = jnp.sum(jnp.where(own, jnp.exp(total), 0.0), axis=0, keepdims=True)
        high = flat.astype(bf16).astype(f32)
        outs[9][:, d * heads : (d + 1) * heads] = high
        outs[9][:, (2 + d) * heads : (3 + d) * heads] = flat - high


def local_kernel(
    value_ref,
    value_before,
    value_after,
    value_weight,
    key_ref,
    key_before,
    key_after,
    key_weight,
    forward_terms,
    backward_terms,
    extra_ref,
    value_out,
    key_out,
    sent_ref,
    wide,
    narrow,
    *,
    heads,
    per_group,
    columns,
):
    group = pl.program_id(0)
    width = value_ref.shape[1]
    values = convolved(value_ref, value_before, value_after, value_weight, wide).astype(bf16)
    value_out[...] = values
    keys = silu(convolved(key_ref, key_before, key_after, key_weight, narrow)).astype(bf16)
    key_out[...] = keys
    for d, terms in ((0, forward_terms), (1, backward_terms)):
        factor = pick_heads(terms[...], heads, group, per_group, HEAD_DIM)
        scaled = (values.astype(f32) * factor).astype(bf16)
        state = lax.dot_general(
            keys, scaled, (((0,), (0,)), ((), ())), preferred_element_type=f32
        )
        start = pl.multiple_of(d * columns + group * width, LANES)
        sent_ref[:, pl.ds(start, width)] = state.astype(bf16)

    @pl.when(group == 0)
    def _():
        sent_ref[:, 2 * columns :] = jnp.broadcast_to(
            extra_ref[...].astype(bf16), (sent_ref.shape[0], extra_ref.shape[1])
        )


def inner_kernel(
    value_ref,
    key_ref,
    query_ref,
    query_before,
    query_after,
    query_weight,
    forward_terms,
    backward_terms,
    forward_row,
    backward_row,
    both_row,
    inner_ref,
    query_out,
    narrow,
    *,
    heads,
    per_group,
):
    group = pl.program_id(0)
    tokens = value_ref.shape[0]
    values = value_ref[...]
    queries = silu(convolved(query_ref, query_before, query_after, query_weight, narrow))
    queries = queries.astype(bf16)
    query_out[...] = queries
    scores = lax.dot_general(
        queries, key_ref[...], (((1,), (1,)), ((), ())), preferred_element_type=f32
    )
    row = lax.broadcasted_iota(jnp.int32, (tokens, tokens), 0)
    column = lax.broadcasted_iota(jnp.int32, (tokens, tokens), 1)
    below, above = row > column, row < column
    forward_columns = pick_heads(forward_terms[...], heads, group, per_group, LANES)
    backward_columns = pick_heads(backward_terms[...], heads, group, per_group, LANES)
    for j in range(per_group):
        lanes = slice(j * LANES, (j + 1) * LANES)
        own = pl.ds(group * per_group + j, 1)
        spread = [forward_columns[:, lanes]] * (tokens // LANES)
        forward = jnp.concatenate(spread, axis=1) - forward_row[own, :]
        spread = [backward_columns[:, lanes]] * (tokens // LANES)
        backward = backward_row[own, :] - jnp.concatenate(spread, axis=1)
        both = jnp.broadcast_to(both_row[own, :], (tokens, tokens))
        exponent = jnp.where(below, forward, jnp.where(above, backward, both))
        weight = (scores * jnp.exp(exponent)).astype(bf16)
        part = slice(j * HEAD_DIM, (j + 1) * HEAD_DIM)
        inner_ref[:, part] = jnp.dot(weight, values[:, part], preferred_element_type=f32)


def carry_kernel(arrived_ref, answer_ref, *, heads, columns):
    count = arrived_ref.shape[0]
    lanes = arrived_ref.shape[2] - 2 * columns
    extra = jnp.concatenate(
        [arrived_ref[k, 0:1, 2 * columns :].astype(f32) for k in range(count)], axis=0
    ).astype(bf16)
    index = lax.broadcasted_iota(jnp.int32, (lanes, 2 * columns), 0)
    column = lax.broadcasted_iota(jnp.int32, (lanes, 2 * columns), 1)
    head = jnp.where(index >= 2 * heads, index - 2 * heads, index)
    wanted = (head == halved(column, columns // heads)) & (index < 4 * heads)
    decays = jnp.dot(extra, wanted.astype(f32).astype(bf16), preferred_element_type=f32)
    forward = slice(0, columns)
    backward = slice(columns, 2 * columns)
    carried = jnp.zeros((arrived_ref.shape[1], columns), f32)
    for k in range(count):
        answer_ref[k, :, forward] = carried.astype(bf16)
        carried = carried * decays[k : k + 1, forward] + arrived_ref[k, :, forward].astype(f32)
    carried = jnp.zeros((arrived_ref.shape[1], columns), f32)
    for k in reversed(range(count)):
        answer_ref[k, :, backward] = carried.astype(bf16)
        carried = carried * decays[k : k + 1, backward] + arrived_ref[k, :, backward].astype(f32)


def output_kernel(
    position_ref,
    query_ref,
    entering_ref,
    leaving_ref,
    inner_ref,
    gate_ref,
    entering_terms,
    leaving_terms,
    gain_ref,
    *rest,
    heads,
    per_group,
    count,
):
    matrices = rest[:count]
    kept_ref, sent_ref, total = rest[-3:]
    group = pl.program_id(0)
    tokens, width = inner_ref.shape
    me = position_ref[0]
    queries = query_ref[...]
    mixed = inner_ref[...]
    for terms, states in ((entering_terms, entering_ref), (leaving_terms, leaving_ref)):
        factor = pick_heads(terms[...], heads, group, per_group, HEAD_DIM)
        mixed = mixed + factor * jnp.dot(queries, states[...], preferred_element_type=f32)
    gated = mixed * silu(gate_ref[...].astype(f32))
    squares = gated * gated
    high = squares.astype(bf16)
    low = (squares - high.astype(f32)).astype(bf16)
    row = lax.broadcasted_iota(jnp.int32, (width, width), 0)
    column = lax.broadcasted_iota(jnp.int32, (width, width), 1)
    same = (halved(row, HEAD_DIM) == halved(column, HEAD_DIM)).astype(f32).astype(bf16)
    mean = jnp.dot(high, same, preferred_element_type=f32)
    mean = (mean + jnp.dot(low, same, preferred_element_type=f32)) * (1.0 / HEAD_DIM)
    normed = (gated * lax.rsqrt(mean + epsilon) * gain_ref[...]).astype(bf16)
    products = [jnp.dot(normed, m[...], preferred_element_type=f32) for m in matrices]
    block = matrices[0].shape[1]

    @pl.when(group == 0)
    def _():
        for t in range(count):
            total[t] = products[t]

    @pl.when(group > 0)
    def _():
        for t in range(count):
            total[t] += products[t]

    @pl.when(group == pl.num_programs(0) - 1)
    def _():
        rows = tokens // count
        for p, r in enumerate(butterfly_order(count)):
            out_ref = kept_ref if 2 * p < count else sent_ref
            place = slice(p % (count // 2) * rows, (p % (count // 2) + 1) * rows)
            first = pl.multiple_of((me ^ r) * rows, SUBLANES)
            for t in range(count):
                start = pl.multiple_of((me ^ t) * block, LANES)
                out_ref[place, pl.ds(start, block)] = total[t, pl.ds(first, rows), :].astype(bf16)


def hold_kernel(*refs):
    count = len(refs) // 3
    copies = [
        pltpu.make_async_copy(refs[k], refs[count + k], refs[2 * count + k]) for k in range(count)
    ]
    for copy in copies:
        copy.start()
    for copy in copies:
        copy.wait()


def held(matrices):
    return pl.pallas_call(
        hold_kernel,
        name="hold",
        in_specs=[pl.BlockSpec(memory_space=pltpu.HBM) for _ in matrices],
        out_specs=[pl.BlockSpec(memory_space=pltpu.VMEM) for _ in matrices],
        out_shape=[jax.ShapeDtypeStruct(m.shape, m.dtype) for m in matrices],
        scratch_shapes=[pltpu.SemaphoreType.DMA for _ in matrices],
        compiler_params=pltpu.CompilerParams(vmem_limit_bytes=16 << 20),
    )(*matrices)


def expert_kernel(*refs):
    *row_refs, gate_ref, up_ref, down_ref, kept_ref, sent_ref = refs
    rows = joined([r[...] for r in row_refs])
    hidden = gate_ref.shape[2]
    tile = min(256, hidden)
    total = None
    for f in range(hidden // tile):
        part = slice(f * tile, (f + 1) * tile)
        gate = jnp.dot(rows, gate_ref[0, :, part], preferred_element_type=f32)
        up = jnp.dot(rows, up_ref[0, :, part], preferred_element_type=f32)
        product = jnp.dot(
            (silu(gate) * up).astype(bf16), down_ref[0, part, :], preferred_element_type=f32
        )
        total = product if total is None else total + product
    half = kept_ref.shape[0]
    kept_ref[...] = total[:half].astype(bf16)
    sent_ref[...] = total[half:].astype(bf16)


def expert_rows(parts, gate_matrix, up_matrix, down_matrix):
    width = parts[0].shape[1]
    count = sum(p.shape[0] for p in parts)
    hidden = gate_matrix.shape[2]
    return pl.pallas_call(
        expert_kernel,
        name="expert_rows",
        in_specs=[pl.BlockSpec(memory_space=pltpu.VMEM)] * (len(parts) + 3),
        out_specs=[pl.BlockSpec(memory_space=pltpu.VMEM)] * 2,
        out_shape=[jax.ShapeDtypeStruct((count // 2, width), bf16)] * 2,
        cost_estimate=pl.CostEstimate(
            flops=6 * count * width * hidden,
            transcendentals=count * hidden,
            bytes_accessed=6 * width * hidden + 4 * count * width,
        ),
        compiler_params=pltpu.CompilerParams(vmem_limit_bytes=30 << 20),
    )(*parts, gate_matrix, up_matrix, down_matrix)


def final_kernel(middle_ref, mixing_ref, *refs):
    *returned, out_ref = refs
    rows = joined([r[...] for r in returned])
    mixing = mixing_ref[...]
    high = mixing.astype(bf16)
    low = (mixing - high.astype(f32)).astype(bf16)
    total = jnp.dot(high, rows, preferred_element_type=f32)
    total = total + jnp.dot(low, rows, preferred_element_type=f32)
    out_ref[...] = (middle_ref[...].astype(f32) + total).astype(bf16)


def mix_tokens(
    value_projected,
    key_projected,
    query_projected,
    output_gate_projected,
    step_projected_raw,
    head_decay_logarithm,
    position_extra_decay,
    value_filter_weight,
    key_filter_weight,
    query_filter_weight,
    head_norm_gain,
    mixer_output_matrix,
):
    tokens, columns = value_projected.shape
    key_width = key_projected.shape[1]
    heads = step_projected_raw.shape[2]
    groups = key_width // STATE
    per_group = heads // groups
    width = per_group * HEAD_DIM
    experts = lax.axis_size("sp")
    count = lax.axis_size("tp")
    before, after = halo_rows([value_projected, key_projected, query_projected])
    early = own_row_block(mixer_output_matrix, columns, count // 2)
    shapes = [(3, heads, tokens)] * 2 + [(2, heads, tokens)] * 4
    shapes = [jax.ShapeDtypeStruct(k, bf16) for k in shapes]
    shapes += [jax.ShapeDtypeStruct((heads, tokens), f32)] * 3
    extra_lanes = -(-4 * heads // LANES) * LANES
    shapes += [jax.ShapeDtypeStruct((1, extra_lanes), f32)]
    outs = pl.pallas_call(
        decay_kernel,
        name="decays",
        out_shape=shapes,
        compiler_params=pltpu.CompilerParams(vmem_limit_bytes=60 * 1024 * 1024),
    )(
        jnp.swapaxes(step_projected_raw, 1, 2),
        head_decay_logarithm,
        position_extra_decay.T,
    )
    terms = [t.reshape(-1, tokens) for t in outs[:6]]
    column_terms, state_terms, read_terms = terms[:2], terms[2:4], terms[4:]
    row_terms = list(outs[6:9])
    extra = outs[9]
    value_blocks, key_blocks = columns // STATE, key_width // STATE

    def whole(x):
        return pl.BlockSpec(x.shape, lambda g: (0,) * x.ndim)

    def columns_of(rows, size, offset):
        return pl.BlockSpec((rows, size), lambda g: (0, offset + g))

    values, keys, sent = pl.pallas_call(
        functools.partial(local_kernel, heads=heads, per_group=per_group, columns=columns),
        name="local_mix",
        grid=(groups,),
        in_specs=[
            columns_of(tokens, width, 0),
            columns_of(HALF, width, 0),
            columns_of(HALF, width, 0),
            columns_of(TAPS, width, 0),
            columns_of(tokens, STATE, 0),
            columns_of(HALF, STATE, value_blocks),
            columns_of(HALF, STATE, value_blocks),
            columns_of(TAPS, STATE, 0),
            whole(state_terms[0]),
            whole(state_terms[1]),
            whole(extra),
        ],
        out_specs=[
            columns_of(tokens, width, 0),
            columns_of(tokens, STATE, 0),
            pl.BlockSpec((STATE, 2 * columns + extra_lanes), lambda g: (0, 0)),
        ],
        out_shape=[
            jax.ShapeDtypeStruct((tokens, columns), bf16),
            jax.ShapeDtypeStruct((tokens, key_width), bf16),
            jax.ShapeDtypeStruct((STATE, 2 * columns + extra_lanes), bf16),
        ],
        scratch_shapes=[
            pltpu.VMEM((tokens + 2 * SUBLANES, width), f32),
            pltpu.VMEM((tokens + 2 * SUBLANES, STATE), f32),
        ],
        compiler_params=pltpu.CompilerParams(
            dimension_semantics=("arbitrary",), vmem_limit_bytes=60 << 20
        ),
    )(
        value_projected,
        before,
        after,
        value_filter_weight,
        key_projected,
        before,
        after,
        key_filter_weight,
        *state_terms,
        extra,
    )
    later_matrix, _ = lax.optimization_barrier((mixer_output_matrix, sent))
    own_columns = [
        early if t == count // 2 else own_row_block(later_matrix, columns, t)
        for t in range(count)
    ]
    inner, queries = pl.pallas_call(
        functools.partial(inner_kernel, heads=heads, per_group=per_group),
        name="inner_mix",
        grid=(groups,),
        in_specs=[
            columns_of(tokens, width, 0),
            columns_of(tokens, STATE, 0),
            columns_of(tokens, STATE, 0),
            columns_of(HALF, STATE, value_blocks + key_blocks),
            columns_of(HALF, STATE, value_blocks + key_blocks),
            columns_of(TAPS, STATE, 0),
        ]
        + [whole(t) for t in column_terms + row_terms],
        out_specs=[columns_of(tokens, width, 0), columns_of(tokens, STATE, 0)],
        out_shape=[
            jax.ShapeDtypeStruct((tokens, columns), f32),
            jax.ShapeDtypeStruct((tokens, key_width), bf16),
        ],
        scratch_shapes=[pltpu.VMEM((tokens + 2 * SUBLANES, STATE), f32)],
        cost_estimate=pl.CostEstimate(
            flops=groups * tokens * tokens * 2 * (STATE + width),
            transcendentals=groups * per_group * tokens * tokens,
            bytes_accessed=8 * tokens * columns,
        ),
        compiler_params=pltpu.CompilerParams(
            dimension_semantics=("arbitrary",), vmem_limit_bytes=60 << 20
        ),
    )(values, keys, query_projected, before, after, query_filter_weight, *column_terms, *row_terms)
    sent = sent.reshape(experts, STATE // experts, sent.shape[1])
    arrived = lax.all_to_all(sent, "sp", split_axis=0, concat_axis=0, tiled=True)
    answer = pl.pallas_call(
        functools.partial(carry_kernel, heads=heads, columns=columns),
        name="carry",
        out_shape=jax.ShapeDtypeStruct((experts, STATE // experts, 2 * columns), bf16),
        compiler_params=pltpu.CompilerParams(vmem_limit_bytes=60 * 1024 * 1024),
    )(arrived)
    states = lax.all_to_all(answer, "sp", split_axis=0, concat_axis=0, tiled=True)
    states = states.reshape(STATE, 2 * columns)
    block = own_columns[0].shape[1]
    position = lax.axis_index("tp").astype(jnp.int32).reshape(1)
    gain = head_norm_gain.reshape(1, columns)
    return pl.pallas_call(
        functools.partial(output_kernel, heads=heads, per_group=per_group, count=count),
        name="mix_output",
        grid=(groups,),
        in_specs=[
            pl.BlockSpec(memory_space=pltpu.SMEM),
            columns_of(tokens, STATE, 0),
            columns_of(STATE, width, 0),
            columns_of(STATE, width, groups),
            columns_of(tokens, width, 0),
            columns_of(tokens, width, 0),
            whole(read_terms[0]),
            whole(read_terms[1]),
            columns_of(1, width, 0),
        ]
        + [pl.BlockSpec((width, block), lambda g: (g, 0)) for _ in own_columns],
        out_specs=[pl.BlockSpec((tokens // 2, count * block), lambda g: (0, 0))] * 2,
        out_shape=[jax.ShapeDtypeStruct((tokens // 2, count * block), bf16)] * 2,
        scratch_shapes=[pltpu.VMEM((count, tokens, block), f32)],
        compiler_params=pltpu.CompilerParams(
            dimension_semantics=("arbitrary",), vmem_limit_bytes=MIX_BYTES
        ),
    )(
        position,
        queries,
        states,
        states,
        inner,
        output_gate_projected,
        *read_terms,
        gain,
        *own_columns,
    )


def slot_table(route_rows, experts, capacity, here):
    flat_ids = route_rows.reshape(-1)
    expert_ids = lax.broadcasted_iota(jnp.int32, (flat_ids.shape[0], experts), 1)
    matches = (flat_ids[:, None] == expert_ids).astype(f32)
    below = prefix_matrix(flat_ids.shape[0]).astype(bf16)
    running = jnp.dot(below, matches.astype(bf16), preferred_element_type=f32)
    rank_in = (jnp.sum(matches * running, axis=1) - 1.0).astype(jnp.int32)
    return ((flat_ids ^ here) * capacity + rank_in).reshape(route_rows.shape)


def own_row_block(matrix, rows, distance):
    block = lax.dynamic_slice_in_dim(matrix, (lax.axis_index("tp") ^ distance) * rows, rows, 0)
    return exchange(block, "tp", distance) if distance else block


def chunks_of(experts):
    quarter = max(experts // 4, 1)
    return [range(k, k + quarter) for k in range(0, experts, quarter)]


def shards(
    residual_layer_input,
    value_projected,
    key_projected,
    query_projected,
    output_gate_projected,
    step_projected_raw,
    head_decay_logarithm,
    position_extra_decay,
    value_filter_weight,
    key_filter_weight,
    query_filter_weight,
    head_norm_gain,
    mixer_output_matrix,
    expert_norm_gain,
    routes,
    chosen_expert_weight,
    expert_gate_matrix,
    expert_up_matrix,
    expert_down_matrix,
):
    experts = lax.axis_size("sp")
    here = lax.axis_index("sp")
    position = lax.axis_index("tp")
    own_rows, model_width = residual_layer_input.shape
    top_count = routes.shape[1]
    capacity = 2 * own_rows * top_count // experts
    places = experts * capacity
    own_routes = lax.dynamic_slice_in_dim(routes, position * own_rows, own_rows, 0)
    own_slots = slot_table(own_routes, experts, capacity, here)
    place_ids = lax.broadcasted_iota(jnp.int32, (places,) + own_slots.shape, 0)
    one_hot = jnp.sum((place_ids == own_slots[None]).astype(f32), axis=2).astype(bf16)
    chosen = (
        lax.broadcasted_iota(jnp.int32, (own_rows, top_count, places), 2) == own_slots[:, :, None]
    )
    mixing = jnp.sum(jnp.where(chosen, chosen_expert_weight[:, :, None], 0.0), axis=1)

    kept, sent = mix_tokens(
        value_projected,
        key_projected,
        query_projected,
        output_gate_projected,
        step_projected_raw,
        head_decay_logarithm,
        position_extra_decay,
        value_filter_weight,
        key_filter_weight,
        query_filter_weight,
        head_norm_gain,
        mixer_output_matrix,
    )
    mixer_out = scatter_rows(kept, sent, "tp")
    middle = add_rounded(residual_layer_input, mixer_out)
    residual = middle.astype(f32)
    normed = (
        residual
        * lax.rsqrt(jnp.mean(residual * residual, axis=-1, keepdims=True) + epsilon)
        * expert_norm_gain
    ).astype(bf16)
    outgoing = jnp.dot(one_hot, normed, preferred_element_type=f32).astype(bf16)
    outgoing = outgoing.reshape(experts, capacity, model_width)
    matrices = held([expert_gate_matrix, expert_up_matrix, expert_down_matrix])
    returned = []
    for chunk in chunks_of(experts):
        arrived = [exchange(outgoing[d], "sp", d) if d else outgoing[d] for d in chunk]
        parts = gather_rows(joined(arrived), "tp")
        halves = expert_rows(parts, *matrices)
        summed = scatter_rows(*halves, "tp")
        results = summed.reshape(len(chunk), capacity, model_width)
        returned += [
            exchange(results[i], "sp", d) if d else results[i] for i, d in enumerate(chunk)
        ]
    if capacity % (2 * SUBLANES):
        returned = [jnp.concatenate(returned, axis=0)]
    return pl.pallas_call(
        final_kernel,
        name="final_mix",
        out_shape=jax.ShapeDtypeStruct(middle.shape, bf16),
        compiler_params=pltpu.CompilerParams(vmem_limit_bytes=16 << 20),
    )(middle, mixing, *returned)


def solution(mesh):
    return jax.shard_map(
        shards,
        mesh=mesh,
        in_specs=(
            P(("sp", "tp"), None),
            P("sp", "tp"),
            P("sp", "tp"),
            P("sp", "tp"),
            P("sp", "tp"),
            P(None, "sp", "tp"),
            P(None, "tp"),
            P("sp", "tp"),
            P(None, "tp"),
            P(None, "tp"),
            P(None, "tp"),
            P("tp"),
            P(None, "tp"),
            P(),
            P("sp", None),
            P(("sp", "tp"), None),
            P("sp", None, "tp"),
            P("sp", None, "tp"),
            P("sp", "tp", None),
        ),
        out_specs=P(("sp", "tp"), None),
        check_vma=False,
    )
```
